512 devices in a mesh: sp: 64 (over z, y), tp: 8 (over x, core).
Axes of the slice: x: 4, y: 8, z: 8, core: 2. Of those that a mesh axis runs over, the one named last changes fastest.
Arguments:
- queries: bfloat16 [1, 24576, 2048], P(None, 'sp', 'tp'), may hold values from -5 to 5
- keys: bfloat16 [1, 24576, 2048], P(None, 'sp', 'tp'), may hold values from -5 to 5
- values: bfloat16 [1, 24576, 2048], P(None, 'sp', 'tp'), may hold values from -6 to 6
- rel_bias: float32 [16, 192], P('tp'), may hold values from -3 to 3
- out_grad: bfloat16 [1, 24576, 2048], P(None, 'sp', 'tp'), may hold values from -48 to 48
Outputs:
- query_grad: bfloat16 [1, 24576, 2048], P(None, 'sp', 'tp')
- key_grad: bfloat16 [1, 24576, 2048], P(None, 'sp', 'tp')
- value_grad: bfloat16 [1, 24576, 2048], P(None, 'sp', 'tp')
- bias_grad: float32 [16, 192], replicated
The draws below stay inside these ranges and needn't reach their ends.
All inputs are finite; a program needn't handle non-finite values.
Results may differ from the reference program's by a relative error of at most 0.0049.
Values may be sent and summed in bfloat16 or wider, within the bound.
No kernel may reach another device: no remote copies, remote signals or barrier semaphores. Data moves between devices by JAX's collectives and lax.ppermute only.
A program may use at most 64 MiB of HBM per device.

```python
import jax
import jax.numpy as jnp
from jax import lax

HEADS = 16
HEAD_DIM = 128
SEG = 64
LEFT = 4
CLIP = 128
SEQS = 1
TOK_DEV = 384
LENGTH = 24576
WIDTH = 2048
BAND = 320
BUCKETS = 192


def aligned_pair(key):
    shape = (SEQS, LENGTH, HEADS * HEAD_DIM)
    base_q = jax.random.normal(jax.random.fold_in(key, 11), shape, jnp.float32)
    base_k = jax.random.normal(jax.random.fold_in(key, 12), shape, jnp.float32)
    return (jnp.clip(base_q, -5.0, 5.0), jnp.clip(base_k, -5.0, 5.0))


def draw_queries(key, part):
    return aligned_pair(key)[0].astype(jnp.bfloat16)


def draw_keys(key, part):
    return aligned_pair(key)[1].astype(jnp.bfloat16)


def steps_of(own_key, dims, pieces, smallest, high):
    def one(dim, blocks):
        heights = jax.random.uniform(jax.random.fold_in(jax.random.fold_in(own_key, 6), dim), (blocks,), jnp.float32, smallest / len(pieces), high / len(pieces))
        return jnp.repeat(jnp.exp(heights), dims[dim] // blocks).reshape((-1,) + (1,) * (len(dims) - dim - 1))

    gain = one(*pieces[0])
    for cut in pieces[1:]:
        gain = gain * one(*cut)
    return gain


def gaussian(rng, shape, width, limit, shards=(), held_as=jnp.bfloat16):
    factor_of = steps_of(rng, shape, shards, -0.22, 0.18) if shards else 1.0
    drawn = jax.random.normal(rng, shape, jnp.float32) * width * factor_of
    return jnp.minimum(jnp.maximum(drawn, -limit), limit).astype(held_as)


def setup_inputs(seed: int = 0) -> dict:
    arg_keys = jax.random.split(jax.random.key(seed), 6)
    queries = draw_queries(jax.random.fold_in(arg_keys[5], 71), 0)
    keys = draw_keys(jax.random.fold_in(arg_keys[5], 71), 0)
    values = gaussian(arg_keys[2], (SEQS, LENGTH, WIDTH), 1.0, 6.0, ((1, 64), (2, 8)))
    rel_bias = gaussian(arg_keys[3], (HEADS, BUCKETS), 0.5, 3.0, ((0, 8),), jnp.float32)
    out_grad = gaussian(arg_keys[4], (SEQS, LENGTH, WIDTH), 8.0, 48.0, ((1, 64), (2, 8)))
    return dict(queries=queries, keys=keys, values=values, rel_bias=rel_bias, out_grad=out_grad)


def relative_index():
    rows = jnp.arange(SEG, dtype=jnp.int32)[:, None] + LEFT * SEG
    cols = jnp.arange(BAND, dtype=jnp.int32)[None, :]
    return (jnp.clip(rows - cols, 1 - SEG, CLIP) + SEG - 1).astype(jnp.int32)


def low_round(array):
    return lax.optimization_barrier(array.astype(jnp.bfloat16)).astype(jnp.float32)


def band_math(q_segs, k_band, v_band, g_segs, table, key_valid):
    seg_count = q_segs.shape[1]
    score_scale = HEAD_DIM ** -0.5
    q_full = q_segs.astype(jnp.float32)
    g_full = g_segs.astype(jnp.float32)
    k_full = k_band.astype(jnp.float32)
    v_full = v_band.astype(jnp.float32)
    score_parts = []
    prob_parts = []
    for offset in range(LEFT + 1):
        score_parts.append(jnp.einsum('sncha,snkha->snhck', q_full, k_full[:, offset:offset + seg_count]))
        prob_parts.append(jnp.einsum('sncha,snkha->snhck', g_full, v_full[:, offset:offset + seg_count]))
    score = jnp.concatenate(score_parts, axis=-1) * score_scale + table[None, None]
    score = jnp.where(key_valid[None, :, None, None, :], score, -jnp.inf)
    row_max = jnp.max(score, axis=-1, keepdims=True)
    expo = jnp.exp(score - row_max)
    prob = expo / jnp.sum(expo, axis=-1, keepdims=True)
    prob_grad = jnp.concatenate(prob_parts, axis=-1)
    row_delta = jnp.sum(prob * prob_grad, axis=-1, keepdims=True)
    score_grad = prob * (prob_grad - row_delta)
    bias_terms = jnp.sum(score_grad, axis=(0, 1))
    prob_low = low_round(prob)
    grad_low = low_round(score_grad * score_scale)
    query_acc = jnp.zeros(q_full.shape, jnp.float32)
    key_acc = jnp.zeros(k_full.shape, jnp.float32)
    value_acc = jnp.zeros(k_full.shape, jnp.float32)
    for offset in range(LEFT + 1):
        grad_part = grad_low[..., offset * SEG:(offset + 1) * SEG]
        prob_part = prob_low[..., offset * SEG:(offset + 1) * SEG]
        query_acc = query_acc + jnp.einsum('snhck,snkha->sncha', grad_part, k_full[:, offset:offset + seg_count])
        key_acc = key_acc.at[:, offset:offset + seg_count].add(jnp.einsum('snhck,sncha->snkha', grad_part, q_full))
        value_acc = value_acc.at[:, offset:offset + seg_count].add(jnp.einsum('snhck,sncha->snkha', prob_part, g_full))
    return query_acc, key_acc, value_acc, bias_terms


def reference(queries, keys, values, rel_bias, out_grad):
    seq_count, length, row_width = queries.shape
    head_count = row_width // HEAD_DIM
    reach = LEFT * SEG
    block_rows = TOK_DEV
    seg_count = block_rows // SEG
    zero_rows = jnp.zeros((seq_count, reach, row_width), keys.dtype)
    keys_pad = jnp.concatenate([zero_rows, keys], axis=1)
    values_pad = jnp.concatenate([zero_rows, values], axis=1)
    rel_ids = relative_index()
    table = jnp.take(rel_bias.astype(jnp.float32), rel_ids, axis=1)
    seg_shape = (seq_count, seg_count, SEG, head_count, HEAD_DIM)
    band_shape = (seq_count, seg_count + LEFT, SEG, head_count, HEAD_DIM)

    def step(carry, block):
        key_sum, value_sum, bias_sum = carry
        start = (block * block_rows).astype(jnp.int32)
        q_blk = lax.dynamic_slice_in_dim(queries, start, block_rows, 1).reshape(seg_shape)
        g_blk = lax.dynamic_slice_in_dim(out_grad, start, block_rows, 1).reshape(seg_shape)
        k_blk = lax.dynamic_slice_in_dim(keys_pad, start, block_rows + reach, 1).reshape(band_shape)
        v_blk = lax.dynamic_slice_in_dim(values_pad, start, block_rows + reach, 1).reshape(band_shape)
        positions = start + jnp.arange(seg_count, dtype=jnp.int32)[:, None] * SEG - reach + jnp.arange(BAND, dtype=jnp.int32)[None, :]
        key_valid = positions >= 0
        query_acc, key_acc, value_acc, bias_terms = band_math(q_blk, k_blk, v_blk, g_blk, table, key_valid)
        flat = (seq_count, block_rows + reach, row_width)
        key_sum = lax.dynamic_update_slice_in_dim(key_sum, lax.dynamic_slice_in_dim(key_sum, start, block_rows + reach, 1) + key_acc.reshape(flat), start, 1)
        value_sum = lax.dynamic_update_slice_in_dim(value_sum, lax.dynamic_slice_in_dim(value_sum, start, block_rows + reach, 1) + value_acc.reshape(flat), start, 1)
        query_out = query_acc.astype(jnp.bfloat16).reshape(seq_count, block_rows, row_width)
        return (key_sum, value_sum, bias_sum + bias_terms), query_out

    init = (jnp.zeros((seq_count, length + reach, row_width), jnp.float32),
            jnp.zeros((seq_count, length + reach, row_width), jnp.float32),
            jnp.zeros((head_count, SEG, BAND), jnp.float32))
    (key_sum, value_sum, bias_sum), query_blocks = lax.scan(step, init, jnp.arange(length // block_rows, dtype=jnp.int32))
    query_grad = jnp.transpose(query_blocks, (1, 0, 2, 3)).reshape(seq_count, length, row_width)
    key_grad = key_sum[:, reach:].astype(jnp.bfloat16)
    value_grad = value_sum[:, reach:].astype(jnp.bfloat16)
    bias_grad = jax.ops.segment_sum(bias_sum.reshape(head_count, -1).T, rel_ids.reshape(-1), num_segments=BUCKETS).T
    return query_grad, key_grad, value_grad, bias_grad
```

```python
import jax
import jax.numpy as jnp
from jax import lax
from jax.experimental import pallas as pl
from jax.experimental.pallas import tpu as pltpu
from jax.sharding import PartitionSpec as P

HEAD_DIM = 128
SEG = 64
LEFT = 4
CLIP = 128
BUCKETS = 192
HEADS = 2
BLK = 128
SCALE = HEAD_DIM**-0.5
LOG2E = 1.4426950408889634
NEG = -1e30
F32 = jnp.float32
BF16 = jnp.bfloat16
VMEM = pl.BlockSpec(memory_space=pltpu.VMEM)
ANY = pl.BlockSpec(memory_space=pl.ANY)


def params(mib):
    return pltpu.CompilerParams(vmem_limit_bytes=mib << 20)


def dot(a, b, ca, cb):
    return lax.dot_general(a, b, (((ca,), (cb,)), ((), ())), preferred_element_type=F32)


def iotas():
    c = lax.broadcasted_iota(jnp.int32, (BLK, BLK), 0)
    r = lax.broadcasted_iota(jnp.int32, (BLK, BLK), 1)
    return c, r


def bias_blocks(row):
    c, r = iotas()
    row = row * LOG2E
    wide = jnp.broadcast_to(row, (8, 2 * BLK))
    mid = pltpu.roll(wide, 2 * BLK - (SEG - 1), 1)[:1, :BLK]
    low = pltpu.roll(wide, SEG + 1, 1)[:1, :BLK]
    top = wide[:1, BUCKETS - 1 : BUCKETS]
    mid = pltpu.roll(jnp.broadcast_to(mid, (BLK, BLK)), 0, 1, stride=1, stride_axis=0)
    low = pltpu.roll(jnp.broadcast_to(low, (BLK, BLK)), 0, 1, stride=1, stride_axis=0)
    t0 = jnp.where((c < SEG) & (r >= SEG), NEG, top)
    t1 = jnp.where(r >= c, top, mid)
    t2 = jnp.where(r >= c, mid, jnp.where((c >= SEG) & (r < SEG), NEG, low))
    return t0, t1, t2


def along_diagonals(x):
    acc = x[:8]
    for a in range(8, BLK, 8):
        acc = acc + pltpu.roll(x[a : a + 8], BLK - a, 1)
    row = lax.broadcasted_iota(jnp.int32, acc.shape, 0)
    for bit in (1, 2, 4):
        acc = jnp.where((row & bit) != 0, pltpu.roll(acc, BLK - bit, 1), acc)
    return jnp.sum(acc, axis=0, keepdims=True)


def skew_sum(d0, d1, d2):
    c, r = iotas()
    upper = r >= c
    mid = along_diagonals(jnp.where(upper, d2, d1))
    low = along_diagonals(jnp.where(upper, 0.0, d2))
    top = jnp.sum(jnp.where(upper, d1, 0.0) + d0, axis=0, keepdims=True)
    top = top + pltpu.roll(jnp.broadcast_to(top, (8, BLK)), SEG, 1)[:1]
    low = jnp.where(r[:1] < SEG, top, low)
    return jnp.concatenate([low, mid], axis=0)


def softmax_grad(scores, prob_grads):
    peak = scores[0].max(axis=0, keepdims=True)
    for s in scores[1:]:
        peak = jnp.maximum(peak, s.max(axis=0, keepdims=True))
    expo = [jnp.exp2(s - peak) for s in scores]
    total = sum(e.sum(axis=0, keepdims=True) for e in expo)
    mixed = sum((e * g).sum(axis=0, keepdims=True) for e, g in zip(expo, prob_grads))
    inv = 1.0 / total
    delta = mixed * inv
    prob = [e * inv for e in expo]
    grad = [p * (g - delta) for p, g in zip(prob, prob_grads)]
    return [p.astype(BF16) for p in prob], [(g * SCALE).astype(BF16) for g in grad], grad


def tails_body(k_ref, v_ref, o_ref, sem):
    rows = o_ref.shape[1]
    first = k_ref.shape[0] - rows
    copies = [
        pltpu.make_async_copy(ref.at[pl.ds(first, rows)], o_ref.at[i], sem.at[i])
        for i, ref in enumerate((k_ref, v_ref))
    ]
    for copy in copies:
        copy.start()
    for copy in copies:
        copy.wait()


def own_body(q_ref, k_ref, v_ref, g_ref, rb_ref, dq_ref, part_ref, pay_ref, tab_ref, rb_pad):
    rb_pad[...] = jnp.zeros_like(rb_pad)
    rb_pad[0:HEADS, 0:BUCKETS] = rb_ref[...]
    for h in range(HEADS):
        hs = slice(h * HEAD_DIM, (h + 1) * HEAD_DIM)
        table = bias_blocks(rb_pad[h : h + 1, :])
        for m in range(3):
            tab_ref[3 * h + m] = table[m]
        k = k_ref[:, hs]
        q = q_ref[2 * BLK :, hs]
        g = g_ref[2 * BLK :, hs]
        raw = dot(k, q, 1, 1)
        dp = dot(v_ref[:, hs], g, 1, 1)
        cut = [slice(m * BLK, (m + 1) * BLK) for m in range(3)]
        scores = [raw[cut[m]] * (SCALE * LOG2E) + table[m] for m in range(3)]
        prob, low, grad = softmax_grad(scores, [dp[cut[m]] for m in range(3)])
        low = jnp.concatenate(low, axis=0)
        dq_ref[:, hs] = dot(low, k, 0, 0).astype(BF16)
        part_ref[0, :, hs] = dot(low, q, 1, 0)
        part_ref[1, :, hs] = dot(jnp.concatenate(prob, axis=0), g, 1, 0)
        pay_ref[2 * h : 2 * h + 2, :] = skew_sum(*grad)


def rest_body(
    q_ref, k_ref, v_ref, g_ref, halo_ref, tab_ref, dq2_ref, part_in, pay_in,
    dq_ref, part_ref, back_ref, pay_ref,
):
    hidden = jnp.where(lax.axis_index("sp") == 0, NEG, 0.0).astype(F32)
    dq_ref[2 * BLK :, :] = dq2_ref[...]
    pay = []
    for h in range(HEADS):
        hs = slice(h * HEAD_DIM, (h + 1) * HEAD_DIM)
        table = [tab_ref[3 * h + m] for m in range(3)]
        ks = [halo_ref[0, :BLK, hs], halo_ref[0, BLK:, hs], k_ref[:BLK, hs], k_ref[BLK : 2 * BLK, hs]]
        vs = [halo_ref[1, :BLK, hs], halo_ref[1, BLK:, hs], v_ref[:BLK, hs], v_ref[BLK : 2 * BLK, hs]]
        q = q_ref[: 2 * BLK, hs]
        g = g_ref[: 2 * BLK, hs]
        lows, probs, sums = [], [], [None] * 3
        for p in range(2):
            rows = slice(p * BLK, (p + 1) * BLK)
            raw = dot(jnp.concatenate(ks[p : p + 3], axis=0), q[rows], 1, 1)
            dp = dot(jnp.concatenate(vs[p : p + 3], axis=0), g[rows], 1, 1)
            cut = [slice(m * BLK, (m + 1) * BLK) for m in range(3)]
            shift = [table[m] + hidden if p + m < 2 else table[m] for m in range(3)]
            scores = [raw[cut[m]] * (SCALE * LOG2E) + shift[m] for m in range(3)]
            prob, low, grad = softmax_grad(scores, [dp[cut[m]] for m in range(3)])
            dq_ref[rows, hs] = dot(
                jnp.concatenate(low, axis=0), jnp.concatenate(ks[p : p + 3], axis=0), 0, 0
            ).astype(BF16)
            lows.append(low)
            probs.append(prob)
            sums = [d if s is None else s + d for s, d in zip(sums, grad)]
        pay.append(skew_sum(*sums))
        for i, (w, x) in enumerate(((lows, q), (probs, g))):
            out = [
                dot(w[0][0], x[:BLK], 1, 0),
                dot(jnp.concatenate([w[0][1], w[1][0]], axis=1), x, 1, 0),
                dot(jnp.concatenate([w[0][2], w[1][1]], axis=1), x, 1, 0),
                dot(w[1][2], x[BLK:], 1, 0),
            ]
            back_ref[i, :BLK, hs] = out[0].astype(BF16)
            back_ref[i, BLK:, hs] = out[1].astype(BF16)
            part_ref[i, :BLK, hs] = part_in[i, :BLK, hs] + out[2]
            part_ref[i, BLK : 2 * BLK, hs] = part_in[i, BLK : 2 * BLK, hs] + out[3]
            part_ref[i, 2 * BLK :, hs] = part_in[i, 2 * BLK :, hs]
    total = jnp.concatenate(pay, axis=0) + pay_in[...]
    pay_ref[...] = jnp.broadcast_to(total[None], pay_ref.shape)


def join_body(part_ref, back_ref, dk_ref, dv_ref):
    for i, out in enumerate((dk_ref, dv_ref)):
        out[:BLK, :] = part_ref[i, :BLK, :].astype(BF16)
        out[BLK:, :] = (part_ref[i, BLK:, :] + back_ref[i].astype(F32)).astype(BF16)


def table_body(x_ref, o_ref):
    heads = o_ref.shape[0]
    low = x_ref[pl.ds(0, heads, stride=2), :]
    mid = x_ref[pl.ds(1, heads, stride=2), :]
    lane = lax.broadcasted_iota(jnp.int32, low.shape, 1)
    top = jnp.sum(jnp.where(lane < SEG, low, 0.0), axis=1, keepdims=True)
    mid = pltpu.roll(mid, SEG - 1, 1)
    first = jnp.where(lane < SEG - 1, pltpu.roll(low, SEG - 1, 1), mid)
    last = jnp.where(lane < SEG - 1, mid, top)
    o_ref[:, :BLK] = first
    o_ref[:, BLK:] = last[:, : BUCKETS - BLK]


def local(queries, keys, values, rel_bias, out_grad):
    _, rows, width = queries.shape
    reach = LEFT * SEG
    q, k, v, g = (a.reshape(rows, width) for a in (queries, keys, values, out_grad))
    count = lax.axis_size("sp")
    heads = lax.axis_size("tp")
    tails = pl.pallas_call(
        tails_body,
        out_shape=jax.ShapeDtypeStruct((2, reach, width), BF16),
        in_specs=[ANY, ANY],
        out_specs=VMEM,
        scratch_shapes=[pltpu.SemaphoreType.DMA((2,))],
        compiler_params=params(4),
        name="tails",
    )(k, v)
    halo = lax.ppermute(tails, "sp", [(s, s + 1) for s in range(count - 1)])
    dq2, part, pay, table = pl.pallas_call(
        own_body,
        out_shape=(
            jax.ShapeDtypeStruct((BLK, width), BF16),
            jax.ShapeDtypeStruct((2, rows, width), F32),
            jax.ShapeDtypeStruct((2 * HEADS, BLK), F32),
            jax.ShapeDtypeStruct((3 * HEADS, BLK, BLK), F32),
        ),
        in_specs=[VMEM] * 5,
        out_specs=(VMEM,) * 4,
        scratch_shapes=[pltpu.VMEM((8, 2 * BLK), F32)],
        compiler_params=params(8),
        name="own",
    )(q, k, v, g, rel_bias)
    dq, part, back, pay = pl.pallas_call(
        rest_body,
        out_shape=(
            jax.ShapeDtypeStruct((rows, width), BF16),
            jax.ShapeDtypeStruct((2, rows, width), F32),
            jax.ShapeDtypeStruct((2, reach, width), BF16),
            jax.ShapeDtypeStruct((count, 2 * HEADS, BLK), F32),
        ),
        in_specs=[VMEM] * 9,
        out_specs=(VMEM,) * 4,
        compiler_params=params(8),
        name="rest",
    )(q, k, v, g, halo, table, dq2, part, pay)
    pay = lax.all_to_all(pay, "sp", split_axis=0, concat_axis=0, tiled=True)
    back = lax.ppermute(back, "sp", [(s + 1, s) for s in range(count - 1)])
    pay = jnp.broadcast_to(jnp.sum(pay, axis=0), (heads, 2 * HEADS, BLK))
    pay = lax.all_to_all(pay, "tp", split_axis=0, concat_axis=0, tiled=True)
    dk, dv = pl.pallas_call(
        join_body,
        out_shape=(jax.ShapeDtypeStruct((rows, width), BF16),) * 2,
        in_specs=[VMEM] * 2,
        out_specs=(VMEM,) * 2,
        compiler_params=params(6),
        name="join",
    )(part, back)
    bias = pl.pallas_call(
        table_body,
        out_shape=jax.ShapeDtypeStruct((heads * HEADS, BUCKETS), F32),
        in_specs=[VMEM],
        out_specs=VMEM,
        compiler_params=params(4),
        name="table",
    )(pay.reshape(heads * 2 * HEADS, BLK))
    return tuple(a.reshape(queries.shape) for a in (dq, dk, dv)) + (bias,)


def solution(mesh):
    return jax.shard_map(
        local,
        mesh=mesh,
        in_specs=(
            P(None, "sp", "tp"),
            P(None, "sp", "tp"),
            P(None, "sp", "tp"),
            P("tp", None),
            P(None, "sp", "tp"),
        ),
        out_specs=(P(None, "sp", "tp"), P(None, "sp", "tp"), P(None, "sp", "tp"), P()),
        check_vma=False,
    )
```

```python
import functools

import jax
import jax.numpy as jnp
from jax import lax
from jax.experimental import pallas as pl
from jax.experimental.pallas import tpu as pltpu
from jax.sharding import Mesh, PartitionSpec as P

HEAD_DIM = 128
SEG = 64
LEFT = 4
CLIP = 128
BUCKETS = 192
HEADS = 2
BLK = 128
SCALE = HEAD_DIM**-0.5
LOG2E = 1.4426950408889634
NEG = -1e30
F32 = jnp.float32
BF16 = jnp.bfloat16
VMEM = pl.BlockSpec(memory_space=pltpu.VMEM)
HBM = pl.BlockSpec(memory_space=pltpu.HBM)
AXES = ("z", "y", "x", "c")


def dot(a, b, ca, cb):
    return lax.dot_general(a, b, (((ca,), (cb,)), ((), ())), preferred_element_type=F32)


def iotas():
    c = lax.broadcasted_iota(jnp.int32, (BLK, BLK), 0)
    r = lax.broadcasted_iota(jnp.int32, (BLK, BLK), 1)
    return c, r


def bias_blocks(row):
    c, r = iotas()
    row = row * LOG2E
    wide = jnp.broadcast_to(row, (8, 2 * BLK))
    mid = pltpu.roll(wide, 2 * BLK - (SEG - 1), 1)[:1, :BLK]
    low = pltpu.roll(wide, SEG + 1, 1)[:1, :BLK]
    top = wide[:1, BUCKETS - 1 : BUCKETS]
    mid = pltpu.roll(jnp.broadcast_to(mid, (BLK, BLK)), 0, 1, stride=1, stride_axis=0)
    low = pltpu.roll(jnp.broadcast_to(low, (BLK, BLK)), 0, 1, stride=1, stride_axis=0)
    t0 = jnp.where((c < SEG) & (r >= SEG), NEG, top)
    t1 = jnp.where(r >= c, top, mid)
    t2 = jnp.where(r >= c, mid, jnp.where((c >= SEG) & (r < SEG), NEG, low))
    return t0, t1, t2


def along_diagonals(x):
    acc = x[:8]
    for a in range(8, BLK, 8):
        acc = acc + pltpu.roll(x[a : a + 8], BLK - a, 1)
    row = lax.broadcasted_iota(jnp.int32, acc.shape, 0)
    for bit in (1, 2, 4):
        acc = jnp.where((row & bit) != 0, pltpu.roll(acc, BLK - bit, 1), acc)
    return jnp.sum(acc, axis=0, keepdims=True)


def skew_sum(d0, d1, d2):
    c, r = iotas()
    upper = r >= c
    mid = along_diagonals(jnp.where(upper, d2, d1))
    low = along_diagonals(jnp.where(upper, 0.0, d2))
    top = jnp.sum(jnp.where(upper, d1, 0.0) + d0, axis=0, keepdims=True)
    top = top + pltpu.roll(jnp.broadcast_to(top, (8, BLK)), SEG, 1)[:1]
    low = jnp.where(r[:1] < SEG, top, low)
    return jnp.concatenate([low, mid], axis=0)


def softmax_grad(expo, prob_grads, inv, delta):
    prob = [e * i for e, i in zip(expo, inv)]
    grad = [p * (g - delta) for p, g in zip(prob, prob_grads)]
    return [p.astype(BF16) for p in prob], [(g * SCALE).astype(BF16) for g in grad], grad


def peak_of(scores):
    return functools.reduce(jnp.maximum, scores).max(axis=0, keepdims=True)


def sum_of(blocks):
    return functools.reduce(jnp.add, blocks).sum(axis=0, keepdims=True)


def weights(scores, prob_grads):
    peak = peak_of(scores)
    expo = [jnp.exp2(s - peak) for s in scores]
    return expo, peak, sum_of(expo), sum_of([e * g for e, g in zip(expo, prob_grads)])


def cut(x):
    return [x[at : at + BLK] for at in range(0, x.shape[0], BLK)]


def stack(blocks):
    return jnp.concatenate(blocks, axis=0)


def head(h):
    return slice(h * HEAD_DIM, (h + 1) * HEAD_DIM)


def hidden_keys():
    first = (lax.axis_index("z") == 0) & (lax.axis_index("y") == 0)
    return jnp.where(first, NEG, 0.0).astype(F32)


def tails_body(k_ref, v_ref, near_ref, far_ref, sem):
    first = k_ref.shape[0] - 2 * BLK
    copies = [
        pltpu.make_async_copy(ref.at[pl.ds(first + at, BLK)], out.at[i], sem.at[2 * i + j])
        for i, ref in enumerate((k_ref, v_ref))
        for j, (out, at) in enumerate(((near_ref, BLK), (far_ref, 0)))
    ]
    for copy in copies:
        copy.start()
    for copy in copies:
        copy.wait()


def own_body(q_ref, k_ref, v_ref, g_ref, rb_ref, dq_ref, mid_ref, end_ref, pay_ref, tab_ref, rb_pad):
    rb_pad[...] = jnp.zeros_like(rb_pad)
    rb_pad[0:HEADS, 0:BUCKETS] = rb_ref[...]
    for h in range(HEADS):
        hs = head(h)
        table = bias_blocks(rb_pad[h : h + 1, :])
        for m in range(3):
            tab_ref[3 * h + m] = table[m]
        k = k_ref[:, hs]
        q = q_ref[2 * BLK :, hs]
        g = g_ref[2 * BLK :, hs]
        scores = [s * (SCALE * LOG2E) + t for s, t in zip(cut(dot(k, q, 1, 1)), table)]
        dp = cut(dot(v_ref[:, hs], g, 1, 1))
        expo, _, total, mixed = weights(scores, dp)
        inv = 1.0 / total
        prob, low, grad = softmax_grad(expo, dp, [inv] * 3, mixed * inv)
        low = stack(low)
        dq_ref[:, hs] = dot(low, k, 0, 0).astype(BF16)
        for i, out in enumerate((dot(low, q, 1, 0), dot(stack(prob), g, 1, 0))):
            mid_ref[i, :, hs] = out[: 2 * BLK]
            end_ref[i, :, hs] = out[2 * BLK :]
        pay_ref[2 * h : 2 * h + 2, :] = skew_sum(*grad)


def near_body(
    q_ref, k_ref, v_ref, g_ref, near_ref, tab_ref, mid_in, pay_in,
    dq_ref, part_ref, pay_ref, expo_ref, dp_ref, stat_ref,
):
    hidden = hidden_keys()
    for h in range(HEADS):
        hs = head(h)
        table = [tab_ref[3 * h + m] for m in range(3)]
        veiled = [table[0] + hidden, table[1] + hidden]
        k = stack([near_ref[0, :, hs], k_ref[: 2 * BLK, hs]])
        v = stack([near_ref[1, :, hs], v_ref[: 2 * BLK, hs]])
        q = q_ref[: 2 * BLK, hs]
        g = g_ref[: 2 * BLK, hs]
        raw = dot(k, q, 1, 1)
        dps = dot(v, g, 1, 1)
        scores = [s * (SCALE * LOG2E) + t for s, t in zip(cut(raw[:, BLK:]), [veiled[0]] + table[1:])]
        dp = cut(dps[:, BLK:])
        expo, _, total, mixed = weights(scores, dp)
        inv = 1.0 / total
        prob, low, grad = softmax_grad(expo, dp, [inv] * 3, mixed * inv)
        low = stack(low)
        dq_ref[:, hs] = dot(low, k, 0, 0).astype(BF16)
        for i, out in enumerate((dot(low, q[BLK:], 1, 0), dot(stack(prob), g[BLK:], 1, 0))):
            part_ref[i, :BLK, hs] = out[:BLK]
            part_ref[i, BLK:, hs] = out[BLK:] + mid_in[i, :, hs]
        pay_ref[2 * h : 2 * h + 2, :] = skew_sum(*grad) + pay_in[2 * h : 2 * h + 2, :]
        scores = [s * (SCALE * LOG2E) + t for s, t in zip(cut(raw[: 2 * BLK, :BLK]), [veiled[1], table[2]])]
        dp = cut(dps[: 2 * BLK, :BLK])
        expo, peak, total, mixed = weights(scores, dp)
        for i in range(2):
            expo_ref[2 * h + i] = expo[i]
            dp_ref[2 * h + i] = dp[i]
        for i, x in enumerate((peak, total, mixed)):
            stat_ref[3 * h + i : 3 * h + i + 1, :] = x


def far_body(
    q_ref, g_ref, far_ref, tab_ref, pay_in, expo_ref, dp_ref, stat_ref, pay_ref, prob_ref, low_ref
):
    hidden = hidden_keys()
    pay = []
    for h in range(HEADS):
        hs = head(h)
        score = dot(far_ref[0, :, hs], q_ref[:BLK, hs], 1, 1) * (SCALE * LOG2E) + (tab_ref[3 * h] + hidden)
        dp = dot(far_ref[1, :, hs], g_ref[:BLK, hs], 1, 1)
        peak, total, mixed = (stat_ref[3 * h + i : 3 * h + i + 1, :] for i in range(3))
        top = jnp.maximum(peak, score.max(axis=0, keepdims=True))
        expo = jnp.exp2(score - top)
        fade = jnp.exp2(peak - top)
        inv = 1.0 / (total * fade + sum_of([expo]))
        delta = (mixed * fade + sum_of([expo * dp])) * inv
        fade = fade * inv
        expos = [expo, expo_ref[2 * h], expo_ref[2 * h + 1]]
        dps = [dp, dp_ref[2 * h], dp_ref[2 * h + 1]]
        prob, low, grad = softmax_grad(expos, dps, [inv, fade, fade], delta)
        pay.append(skew_sum(*grad))
        for m in range(3):
            prob_ref[h, m * BLK : (m + 1) * BLK, :] = prob[m]
            low_ref[h, m * BLK : (m + 1) * BLK, :] = low[m]
    total = jnp.concatenate(pay, axis=0) + pay_in[...]
    pay_ref[...] = jnp.broadcast_to(total[None], pay_ref.shape)


def first_body(
    q_ref, k_ref, g_ref, near_ref, far_ref, part_ref, prob_ref, low_ref, dq1_ref, dq2_ref,
    dq_ref, back_ref, done_ref,
):
    dq_ref[BLK : 2 * BLK, :] = dq1_ref[...]
    dq_ref[2 * BLK :, :] = dq2_ref[...]
    for h in range(HEADS):
        hs = head(h)
        low = low_ref[h]
        keys = stack([far_ref[0, :, hs], near_ref[0, :, hs], k_ref[:BLK, hs]])
        dq_ref[:BLK, hs] = dot(low, keys, 0, 0).astype(BF16)
        outs = (dot(low, q_ref[:BLK, hs], 1, 0), dot(prob_ref[h], g_ref[:BLK, hs], 1, 0))
        for i, out in enumerate(outs):
            back_ref[i, :BLK, hs] = out[:BLK].astype(BF16)
            back_ref[i, BLK:, hs] = (out[BLK : 2 * BLK] + part_ref[i, :BLK, hs]).astype(BF16)
            done_ref[i, :, hs] = (out[2 * BLK :] + part_ref[i, BLK : 2 * BLK, hs]).astype(BF16)


def join_body(part_ref, end_ref, done_ref, back_ref, dk_ref, dv_ref):
    for i, out in enumerate((dk_ref, dv_ref)):
        out[:BLK, :] = done_ref[i]
        out[BLK : 2 * BLK, :] = (part_ref[i, 2 * BLK :, :] + back_ref[i, :BLK, :].astype(F32)).astype(BF16)
        out[2 * BLK :, :] = (end_ref[i] + back_ref[i, BLK:, :].astype(F32)).astype(BF16)


def table_body(x_ref, o_ref, sum_ref):
    heads = o_ref.shape[0]
    sum_ref[...] = jnp.sum(x_ref[...], axis=0)
    low = sum_ref[pl.ds(0, heads, stride=2), :]
    mid = sum_ref[pl.ds(1, heads, stride=2), :]
    lane = lax.broadcasted_iota(jnp.int32, low.shape, 1)
    top = jnp.sum(jnp.where(lane < SEG, low, 0.0), axis=1, keepdims=True)
    mid = pltpu.roll(mid, SEG - 1, 1)
    first = jnp.where(lane < SEG - 1, pltpu.roll(low, SEG - 1, 1), mid)
    last = jnp.where(lane < SEG - 1, mid, top)
    o_ref[:, :BLK] = first
    o_ref[:, BLK:] = last[:, : BUCKETS - BLK]


def call(body, name, outs, args, spaces=None, scratch=(), mib=8):
    return pl.pallas_call(
        body,
        out_shape=tuple(jax.ShapeDtypeStruct(*o) for o in outs),
        in_specs=spaces or [VMEM] * len(args),
        out_specs=(VMEM,) * len(outs),
        scratch_shapes=scratch,
        compiler_params=pltpu.CompilerParams(vmem_limit_bytes=mib << 20),
        name=name,
    )(*args)


def exchange(x, axes):
    return lax.all_to_all(x, axes, split_axis=0, concat_axis=0, tiled=True)


def local(queries, keys, values, rel_bias, out_grad):
    _, rows, width = queries.shape
    q, k, v, g = (a.reshape(rows, width) for a in (queries, keys, values, out_grad))
    size = {a: lax.axis_size(a) for a in AXES}
    count = size["z"] * size["y"]
    pair = (2, BLK, width)
    near, far = call(
        tails_body, "tails", [(pair, BF16)] * 2, (k, v), [HBM] * 2, [pltpu.SemaphoreType.DMA((4,))], 4
    )
    ahead = [(s, s + 1) for s in range(count - 1)]
    near = lax.ppermute(near, ("z", "y"), ahead)
    far = lax.ppermute(far, ("z", "y"), ahead)
    dq2, mid, end, pay, table = call(
        own_body,
        "own",
        [
            ((BLK, width), BF16),
            ((2, 2 * BLK, width), F32),
            (pair, F32),
            ((2 * HEADS, BLK), F32),
            ((3 * HEADS, BLK, BLK), F32),
        ],
        (q, k, v, g, rel_bias),
        scratch=[pltpu.VMEM((8, 2 * BLK), F32)],
    )
    dq1, part, pay, expo, dp, stat = call(
        near_body,
        "near",
        [
            ((BLK, width), BF16),
            ((2, 3 * BLK, width), F32),
            ((2 * HEADS, BLK), F32),
            ((2 * HEADS, BLK, BLK), F32),
            ((2 * HEADS, BLK, BLK), F32),
            ((8, BLK), F32),
        ],
        (q, k, v, g, near, table, mid, pay),
    )
    group = size["y"] * size["c"]
    pay, prob, low = call(
        far_body,
        "far",
        [
            ((group, 2 * HEADS, BLK), F32),
            ((HEADS, 3 * BLK, BLK), BF16),
            ((HEADS, 3 * BLK, BLK), BF16),
        ],
        (q, g, far, table, pay, expo, dp, stat),
    )
    pay = exchange(pay, ("y", "c"))
    dq, back, done = call(
        first_body,
        "first",
        [((rows, width), BF16), ((2, 2 * BLK, width), BF16), (pair, BF16)],
        (q, k, g, near, far, part, prob, low, dq1, dq2),
    )
    back = lax.ppermute(back, ("z", "y"), [(s + 1, s) for s in range(count - 1)])
    pay = pay.reshape(size["y"], size["c"] * 2 * HEADS, BLK).sum(axis=0)
    pay = jnp.broadcast_to(pay, (size["z"] * size["x"], *pay.shape))
    pay = exchange(pay, ("z", "x"))
    dk, dv = call(join_body, "join", [((rows, width), BF16)] * 2, (part, end, done, back), mib=6)
    shape = (size["x"] * size["c"] * 2 * HEADS, BLK)
    (bias,) = call(
        table_body,
        "table",
        [((shape[0] // 2, BUCKETS), F32)],
        (pay.reshape(size["z"], *shape),),
        scratch=[pltpu.VMEM(shape, F32)],
        mib=4,
    )
    return tuple(a.reshape(queries.shape) for a in (dq, dk, dv)) + (bias,)


def solution(mesh):
    sp, tp = mesh.devices.shape
    split = Mesh(mesh.devices.reshape(8, sp // 8, tp // 2, 2), AXES)
    rows = P(None, ("z", "y"), ("x", "c"))
    return jax.shard_map(
        local,
        mesh=split,
        in_specs=(rows, rows, rows, P(("x", "c"), None), rows),
        out_specs=(rows, rows, rows, P()),
        check_vma=False,
    )
```

```python
import functools

import jax
import jax.numpy as jnp
from jax import lax
from jax.experimental import pallas as pl
from jax.experimental.pallas import tpu as pltpu
from jax.sharding import Mesh, PartitionSpec as P

HEAD_DIM = 128
SEG = 64
LEFT = 4
CLIP = 128
BUCKETS = 192
HEADS = 2
BLK = 128
SCALE = HEAD_DIM**-0.5
LOG2E = 1.4426950408889634
NEG = -1e30
F32 = jnp.float32
BF16 = jnp.bfloat16
VMEM = pl.BlockSpec(memory_space=pltpu.VMEM)
HBM = pl.BlockSpec(memory_space=pltpu.HBM)
AXES = ("z", "y", "x", "c")


def dot(a, b, ca, cb):
    return lax.dot_general(a, b, (((ca,), (cb,)), ((), ())), preferred_element_type=F32)


def iotas():
    c = lax.broadcasted_iota(jnp.int32, (BLK, BLK), 0)
    r = lax.broadcasted_iota(jnp.int32, (BLK, BLK), 1)
    return c, r


def bias_blocks(row):
    c, r = iotas()
    row = row * LOG2E
    wide = jnp.broadcast_to(row, (8, 2 * BLK))
    mid = pltpu.roll(wide, 2 * BLK - (SEG - 1), 1)[:1, :BLK]
    low = pltpu.roll(wide, SEG + 1, 1)[:1, :BLK]
    top = wide[:1, BUCKETS - 1 : BUCKETS]
    mid = pltpu.roll(jnp.broadcast_to(mid, (BLK, BLK)), 0, 1, stride=1, stride_axis=0)
    low = pltpu.roll(jnp.broadcast_to(low, (BLK, BLK)), 0, 1, stride=1, stride_axis=0)
    t0 = jnp.where((c < SEG) & (r >= SEG), NEG, top)
    t1 = jnp.where(r >= c, top, mid)
    t2 = jnp.where(r >= c, mid, jnp.where((c >= SEG) & (r < SEG), NEG, low))
    return t0, t1, t2


def along_diagonals(x):
    acc = x[:8]
    for a in range(8, BLK, 8):
        acc = acc + pltpu.roll(x[a : a + 8], BLK - a, 1)
    row = lax.broadcasted_iota(jnp.int32, acc.shape, 0)
    for bit in (1, 2, 4):
        acc = jnp.where((row & bit) != 0, pltpu.roll(acc, BLK - bit, 1), acc)
    return jnp.sum(acc, axis=0, keepdims=True)


def skew_sum(d0, d1, d2):
    c, r = iotas()
    upper = r >= c
    mid = along_diagonals(jnp.where(upper, d2, d1))
    low = along_diagonals(jnp.where(upper, 0.0, d2))
    top = jnp.sum(jnp.where(upper, d1, 0.0) + d0, axis=0, keepdims=True)
    top = top + pltpu.roll(jnp.broadcast_to(top, (8, BLK)), SEG, 1)[:1]
    low = jnp.where(r[:1] < SEG, top, low)
    return jnp.concatenate([low, mid], axis=0)


def softmax_grad(expo, prob_grads, inv, delta):
    prob = [e * i for e, i in zip(expo, inv)]
    grad = [p * (g - delta) for p, g in zip(prob, prob_grads)]
    return [p.astype(BF16) for p in prob], [(g * SCALE).astype(BF16) for g in grad], grad


def peak_of(scores):
    return functools.reduce(jnp.maximum, scores).max(axis=0, keepdims=True)


def sum_of(blocks):
    return functools.reduce(jnp.add, blocks).sum(axis=0, keepdims=True)


def weights(scores, prob_grads):
    peak = peak_of(scores)
    expo = [jnp.exp2(s - peak) for s in scores]
    return expo, peak, sum_of(expo), sum_of([e * g for e, g in zip(expo, prob_grads)])


def cut(x):
    return [x[at : at + BLK] for at in range(0, x.shape[0], BLK)]


def stack(blocks):
    return jnp.concatenate(blocks, axis=0)


def head(h):
    return slice(h * HEAD_DIM, (h + 1) * HEAD_DIM)


def hidden_keys():
    first = (lax.axis_index("z") == 0) & (lax.axis_index("y") == 0)
    return jnp.where(first, NEG, 0.0).astype(F32)


def tails_body(k_ref, v_ref, near_ref, far_ref, sem):
    first = k_ref.shape[0] - 2 * BLK
    copies = [
        pltpu.make_async_copy(ref.at[pl.ds(first + at, BLK)], out.at[i], sem.at[2 * i + j])
        for i, ref in enumerate((k_ref, v_ref))
        for j, (out, at) in enumerate(((near_ref, BLK), (far_ref, 0)))
    ]
    for copy in copies:
        copy.start()
    for copy in copies:
        copy.wait()


def own_body(q_ref, k_ref, v_ref, g_ref, rb_ref, dq_ref, mid_ref, end_ref, pay_ref, tab_ref, rb_pad):
    rb_pad[...] = jnp.zeros_like(rb_pad)
    rb_pad[0:HEADS, 0:BUCKETS] = rb_ref[...]
    for h in range(HEADS):
        hs = head(h)
        table = bias_blocks(rb_pad[h : h + 1, :])
        for m in range(3):
            tab_ref[3 * h + m] = table[m]
        k = k_ref[:, hs]
        q = q_ref[2 * BLK :, hs]
        g = g_ref[2 * BLK :, hs]
        scores = [s * (SCALE * LOG2E) + t for s, t in zip(cut(dot(k, q, 1, 1)), table)]
        dp = cut(dot(v_ref[:, hs], g, 1, 1))
        expo, _, total, mixed = weights(scores, dp)
        inv = 1.0 / total
        prob, low, grad = softmax_grad(expo, dp, [inv] * 3, mixed * inv)
        low = stack(low)
        dq_ref[:, hs] = dot(low, k, 0, 0).astype(BF16)
        for i, out in enumerate((dot(low, q, 1, 0), dot(stack(prob), g, 1, 0))):
            mid_ref[i, :, hs] = out[: 2 * BLK]
            end_ref[i, :, hs] = out[2 * BLK :]
        pay_ref[2 * h : 2 * h + 2, :] = skew_sum(*grad)


def near_body(
    q_ref, k_ref, v_ref, g_ref, near_ref, tab_ref, mid_in, pay_in,
    dq_ref, part_ref, pay_ref, expo_ref, dp_ref, stat_ref,
):
    hidden = hidden_keys()
    for h in range(HEADS):
        hs = head(h)
        table = [tab_ref[3 * h + m] for m in range(3)]
        veiled = [table[0] + hidden, table[1] + hidden]
        k = stack([near_ref[0, :, hs], k_ref[: 2 * BLK, hs]])
        v = stack([near_ref[1, :, hs], v_ref[: 2 * BLK, hs]])
        q = q_ref[: 2 * BLK, hs]
        g = g_ref[: 2 * BLK, hs]
        raw = dot(k, q, 1, 1)
        dps = dot(v, g, 1, 1)
        scores = [s * (SCALE * LOG2E) + t for s, t in zip(cut(raw[:, BLK:]), [veiled[0]] + table[1:])]
        dp = cut(dps[:, BLK:])
        expo, _, total, mixed = weights(scores, dp)
        inv = 1.0 / total
        prob, low, grad = softmax_grad(expo, dp, [inv] * 3, mixed * inv)
        low = stack(low)
        dq_ref[:, hs] = dot(low, k, 0, 0).astype(BF16)
        for i, out in enumerate((dot(low, q[BLK:], 1, 0), dot(stack(prob), g[BLK:], 1, 0))):
            part_ref[i, :BLK, hs] = out[:BLK]
            part_ref[i, BLK:, hs] = out[BLK:] + mid_in[i, :, hs]
        pay_ref[2 * h : 2 * h + 2, :] = skew_sum(*grad) + pay_in[2 * h : 2 * h + 2, :]
        scores = [s * (SCALE * LOG2E) + t for s, t in zip(cut(raw[: 2 * BLK, :BLK]), [veiled[1], table[2]])]
        dp = cut(dps[: 2 * BLK, :BLK])
        expo, peak, total, mixed = weights(scores, dp)
        for i in range(2):
            expo_ref[2 * h + i] = expo[i]
            dp_ref[2 * h + i] = dp[i]
        for i, x in enumerate((peak, total, mixed)):
            stat_ref[3 * h + i : 3 * h + i + 1, :] = x


def far_body(
    q_ref, g_ref, far_ref, tab_ref, pay_in, expo_ref, dp_ref, stat_ref, pay_ref, prob_ref, low_ref
):
    hidden = hidden_keys()
    pay = []
    for h in range(HEADS):
        hs = head(h)
        score = dot(far_ref[0, :, hs], q_ref[:BLK, hs], 1, 1) * (SCALE * LOG2E) + (tab_ref[3 * h] + hidden)
        dp = dot(far_ref[1, :, hs], g_ref[:BLK, hs], 1, 1)
        peak, total, mixed = (stat_ref[3 * h + i : 3 * h + i + 1, :] for i in range(3))
        top = jnp.maximum(peak, score.max(axis=0, keepdims=True))
        expo = jnp.exp2(score - top)
        fade = jnp.exp2(peak - top)
        inv = 1.0 / (total * fade + sum_of([expo]))
        delta = (mixed * fade + sum_of([expo * dp])) * inv
        fade = fade * inv
        expos = [expo, expo_ref[2 * h], expo_ref[2 * h + 1]]
        dps = [dp, dp_ref[2 * h], dp_ref[2 * h + 1]]
        prob, low, grad = softmax_grad(expos, dps, [inv, fade, fade], delta)
        pay.append(skew_sum(*grad))
        for m in range(3):
            prob_ref[h, m * BLK : (m + 1) * BLK, :] = prob[m]
            low_ref[h, m * BLK : (m + 1) * BLK, :] = low[m]
    total = jnp.concatenate(pay, axis=0) + pay_in[...]
    pay_ref[...] = jnp.broadcast_to(total[None], pay_ref.shape)


def first_body(
    q_ref, k_ref, g_ref, near_ref, far_ref, part_ref, prob_ref, low_ref, dq1_ref, dq2_ref,
    dq_ref, back_ref, done_ref,
):
    dq_ref[BLK : 2 * BLK, :] = dq1_ref[...]
    dq_ref[2 * BLK :, :] = dq2_ref[...]
    for h in range(HEADS):
        hs = head(h)
        low = low_ref[h]
        keys = stack([far_ref[0, :, hs], near_ref[0, :, hs], k_ref[:BLK, hs]])
        dq_ref[:BLK, hs] = dot(low, keys, 0, 0).astype(BF16)
        outs = (dot(low, q_ref[:BLK, hs], 1, 0), dot(prob_ref[h], g_ref[:BLK, hs], 1, 0))
        for i, out in enumerate(outs):
            back_ref[i, :BLK, hs] = out[:BLK].astype(BF16)
            back_ref[i, BLK:, hs] = (out[BLK : 2 * BLK] + part_ref[i, :BLK, hs]).astype(BF16)
            done_ref[i, :, hs] = (out[2 * BLK :] + part_ref[i, BLK : 2 * BLK, hs]).astype(BF16)


def join_body(part_ref, end_ref, done_ref, back_ref, dk_ref, dv_ref):
    for i, out in enumerate((dk_ref, dv_ref)):
        out[:BLK, :] = done_ref[i]
        out[BLK : 2 * BLK, :] = (part_ref[i, 2 * BLK :, :] + back_ref[i, :BLK, :].astype(F32)).astype(BF16)
        out[2 * BLK :, :] = (end_ref[i] + back_ref[i, BLK:, :].astype(F32)).astype(BF16)


def table_body(x_ref, o_ref, sum_ref):
    heads = o_ref.shape[0]
    sum_ref[...] = jnp.sum(x_ref[...], axis=0)
    low = sum_ref[pl.ds(0, heads, stride=2), :]
    mid = sum_ref[pl.ds(1, heads, stride=2), :]
    lane = lax.broadcasted_iota(jnp.int32, low.shape, 1)
    top = jnp.sum(jnp.where(lane < SEG, low, 0.0), axis=1, keepdims=True)
    mid = pltpu.roll(mid, SEG - 1, 1)
    first = jnp.where(lane < SEG - 1, pltpu.roll(low, SEG - 1, 1), mid)
    last = jnp.where(lane < SEG - 1, mid, top)
    o_ref[:, :BLK] = first
    o_ref[:, BLK:] = last[:, : BUCKETS - BLK]


def call(body, name, outs, args, spaces=None, scratch=(), mib=8):
    return pl.pallas_call(
        body,
        out_shape=tuple(jax.ShapeDtypeStruct(*o) for o in outs),
        in_specs=spaces or [VMEM] * len(args),
        out_specs=(VMEM,) * len(outs),
        scratch_shapes=scratch,
        compiler_params=pltpu.CompilerParams(vmem_limit_bytes=mib << 20),
        name=name,
    )(*args)


def exchange(x, axes):
    return lax.all_to_all(x, axes, split_axis=0, concat_axis=0, tiled=True)


def local(queries, keys, values, rel_bias, out_grad):
    _, rows, width = queries.shape
    q, k, v, g = (a.reshape(rows, width) for a in (queries, keys, values, out_grad))
    size = {a: lax.axis_size(a) for a in AXES}
    count = size["z"] * size["y"]
    pair = (2, BLK, width)
    kept = tuple(pltpu.with_memory_space_constraint(a, pltpu.HBM) for a in (k, v))
    near, far = call(
        tails_body, "tails", [(pair, BF16)] * 2, kept, [HBM] * 2, [pltpu.SemaphoreType.DMA((4,))], 4
    )
    ahead = [(s, s + 1) for s in range(count - 1)]
    near = lax.ppermute(near, ("z", "y"), ahead)
    far = lax.ppermute(far, ("z", "y"), ahead)
    dq2, mid, end, pay, table = call(
        own_body,
        "own",
        [
            ((BLK, width), BF16),
            ((2, 2 * BLK, width), F32),
            (pair, F32),
            ((2 * HEADS, BLK), F32),
            ((3 * HEADS, BLK, BLK), F32),
        ],
        (q, k, v, g, rel_bias),
        scratch=[pltpu.VMEM((8, 2 * BLK), F32)],
    )
    dq1, part, pay, expo, dp, stat = call(
        near_body,
        "near",
        [
            ((BLK, width), BF16),
            ((2, 3 * BLK, width), F32),
            ((2 * HEADS, BLK), F32),
            ((2 * HEADS, BLK, BLK), F32),
            ((2 * HEADS, BLK, BLK), F32),
            ((8, BLK), F32),
        ],
        (q, k, v, g, near, table, mid, pay),
    )
    group = size["y"] * size["c"]
    pay, prob, low = call(
        far_body,
        "far",
        [
            ((group, 2 * HEADS, BLK), F32),
            ((HEADS, 3 * BLK, BLK), BF16),
            ((HEADS, 3 * BLK, BLK), BF16),
        ],
        (q, g, far, table, pay, expo, dp, stat),
    )
    pay = exchange(pay, ("y", "c"))
    dq, back, done = call(
        first_body,
        "first",
        [((rows, width), BF16), ((2, 2 * BLK, width), BF16), (pair, BF16)],
        (q, k, g, near, far, part, prob, low, dq1, dq2),
    )
    back = lax.ppermute(back, ("z", "y"), [(s + 1, s) for s in range(count - 1)])
    pay = pay.reshape(size["y"], size["c"] * 2 * HEADS, BLK).sum(axis=0)
    pay = jnp.broadcast_to(pay, (size["z"] * size["x"], *pay.shape))
    pay = exchange(pay, ("z", "x"))
    dk, dv = call(join_body, "join", [((rows, width), BF16)] * 2, (part, end, done, back), mib=6)
    shape = (size["x"] * size["c"] * 2 * HEADS, BLK)
    (bias,) = call(
        table_body,
        "table",
        [((shape[0] // 2, BUCKETS), F32)],
        (pay.reshape(size["z"], *shape),),
        scratch=[pltpu.VMEM(shape, F32)],
        mib=4,
    )
    return tuple(a.reshape(queries.shape) for a in (dq, dk, dv)) + (bias,)


def solution(mesh):
    sp, tp = mesh.devices.shape
    split = Mesh(mesh.devices.reshape(8, sp // 8, tp // 2, 2), AXES)
    rows = P(None, ("z", "y"), ("x", "c"))
    return jax.shard_map(
        local,
        mesh=split,
        in_specs=(rows, rows, rows, P(("x", "c"), None), rows),
        out_specs=(rows, rows, rows, P()),
        check_vma=False,
    )
```

```python
import functools
import math

import jax
import jax.numpy as jnp
from jax import lax
from jax.experimental import pallas as pl
from jax.experimental.pallas import tpu as pltpu
from jax.sharding import Mesh, PartitionSpec as P

HEAD_DIM = 128
SEG = 64
LEFT = 4
CLIP = 128
BUCKETS = 192
HEADS = 2
BLK = 128
SCALE = HEAD_DIM**-0.5
LOG2E = 1.4426950408889634
NEG = -1e30
F32 = jnp.float32
BF16 = jnp.bfloat16
VMEM = pl.BlockSpec(memory_space=pltpu.VMEM)
HBM = pl.BlockSpec(memory_space=pltpu.HBM)
AXES = ("z", "y", "x", "c")


def dot(a, b, ca, cb):
    return lax.dot_general(a, b, (((ca,), (cb,)), ((), ())), preferred_element_type=F32)


def iotas():
    c = lax.broadcasted_iota(jnp.int32, (BLK, BLK), 0)
    r = lax.broadcasted_iota(jnp.int32, (BLK, BLK), 1)
    return c, r


def bias_blocks(row):
    c, r = iotas()
    row = row * LOG2E
    wide = jnp.broadcast_to(row, (8, 2 * BLK))
    mid = pltpu.roll(wide, 2 * BLK - (SEG - 1), 1)[:1, :BLK]
    low = pltpu.roll(wide, SEG + 1, 1)[:1, :BLK]
    top = wide[:1, BUCKETS - 1 : BUCKETS]
    mid = pltpu.roll(jnp.broadcast_to(mid, (BLK, BLK)), 0, 1, stride=1, stride_axis=0)
    low = pltpu.roll(jnp.broadcast_to(low, (BLK, BLK)), 0, 1, stride=1, stride_axis=0)
    t0 = jnp.where((c < SEG) & (r >= SEG), NEG, top)
    t1 = jnp.where(r >= c, top, mid)
    t2 = jnp.where(r >= c, mid, jnp.where((c >= SEG) & (r < SEG), NEG, low))
    return t0, t1, t2


def along_diagonals(x):
    acc = x[:8]
    for a in range(8, BLK, 8):
        acc = acc + pltpu.roll(x[a : a + 8], BLK - a, 1)
    row = lax.broadcasted_iota(jnp.int32, acc.shape, 0)
    for bit in (1, 2, 4):
        acc = jnp.where((row & bit) != 0, pltpu.roll(acc, BLK - bit, 1), acc)
    return jnp.sum(acc, axis=0, keepdims=True)


def skew_sum(d0, d1, d2):
    c, r = iotas()
    upper = r >= c
    mid = along_diagonals(jnp.where(upper, d2, d1))
    low = along_diagonals(jnp.where(upper, 0.0, d2))
    top = jnp.sum(jnp.where(upper, d1, 0.0) + d0, axis=0, keepdims=True)
    top = top + pltpu.roll(jnp.broadcast_to(top, (8, BLK)), SEG, 1)[:1]
    low = jnp.where(r[:1] < SEG, top, low)
    return jnp.concatenate([low, mid], axis=0)


def softmax_grad(expo, prob_grads, inv, delta):
    prob = [e * i for e, i in zip(expo, inv)]
    grad = [p * (g - delta) for p, g in zip(prob, prob_grads)]
    return [p.astype(BF16) for p in prob], [(g * SCALE).astype(BF16) for g in grad], grad


def peak_of(scores):
    return functools.reduce(jnp.maximum, scores).max(axis=0, keepdims=True)


def sum_of(blocks):
    return functools.reduce(jnp.add, blocks).sum(axis=0, keepdims=True)


def weights(scores, prob_grads):
    peak = peak_of(scores)
    expo = [jnp.exp2(s - peak) for s in scores]
    return expo, peak, sum_of(expo), sum_of([e * g for e, g in zip(expo, prob_grads)])


def cut(x):
    return [x[at : at + BLK] for at in range(0, x.shape[0], BLK)]


def stack(blocks):
    return jnp.concatenate(blocks, axis=0)


def head(h):
    return slice(h * HEAD_DIM, (h + 1) * HEAD_DIM)


def hidden_keys():
    first = (lax.axis_index("z") == 0) & (lax.axis_index("y") == 0)
    return jnp.where(first, NEG, 0.0).astype(F32)


def tails_body(k_ref, v_ref, near_ref, far_ref, sem):
    first = k_ref.shape[0] - 2 * BLK
    copies = [
        pltpu.make_async_copy(ref.at[pl.ds(first + at, BLK)], out.at[i], sem.at[2 * i + j])
        for i, ref in enumerate((k_ref, v_ref))
        for j, (out, at) in enumerate(((near_ref, BLK), (far_ref, 0)))
    ]
    for copy in copies:
        copy.start()
    for copy in copies:
        copy.wait()


def own_body(q_ref, k_ref, v_ref, g_ref, rb_ref, dq_ref, mid_ref, end_ref, pay_ref, tab_ref, rb_pad):
    rb_pad[...] = jnp.zeros_like(rb_pad)
    rb_pad[0:HEADS, 0:BUCKETS] = rb_ref[...]
    for h in range(HEADS):
        hs = head(h)
        table = bias_blocks(rb_pad[h : h + 1, :])
        for m in range(3):
            tab_ref[3 * h + m] = table[m]
        k = k_ref[:, hs]
        q = q_ref[2 * BLK :, hs]
        g = g_ref[2 * BLK :, hs]
        scores = [s * (SCALE * LOG2E) + t for s, t in zip(cut(dot(k, q, 1, 1)), table)]
        dp = cut(dot(v_ref[:, hs], g, 1, 1))
        expo, _, total, mixed = weights(scores, dp)
        inv = 1.0 / total
        prob, low, grad = softmax_grad(expo, dp, [inv] * 3, mixed * inv)
        low = stack(low)
        dq_ref[:, hs] = dot(low, k, 0, 0).astype(BF16)
        for i, out in enumerate((dot(low, q, 1, 0), dot(stack(prob), g, 1, 0))):
            mid_ref[i, :, hs] = out[: 2 * BLK]
            end_ref[i, :, hs] = out[2 * BLK :]
        pay_ref[2 * h : 2 * h + 2, :] = skew_sum(*grad)


def near_body(
    q_ref, k_ref, v_ref, g_ref, near_ref, tab_ref, mid_in, pay_in,
    dq_ref, part_ref, pay_ref, expo_ref, dp_ref, stat_ref,
):
    hidden = hidden_keys()
    for h in range(HEADS):
        hs = head(h)
        table = [tab_ref[3 * h + m] for m in range(3)]
        veiled = [table[0] + hidden, table[1] + hidden]
        k = stack([near_ref[0, :, hs], k_ref[: 2 * BLK, hs]])
        v = stack([near_ref[1, :, hs], v_ref[: 2 * BLK, hs]])
        q = q_ref[: 2 * BLK, hs]
        g = g_ref[: 2 * BLK, hs]
        raw = dot(k, q, 1, 1)
        dps = dot(v, g, 1, 1)
        scores = [s * (SCALE * LOG2E) + t for s, t in zip(cut(raw[:, BLK:]), [veiled[0]] + table[1:])]
        dp = cut(dps[:, BLK:])
        expo, _, total, mixed = weights(scores, dp)
        inv = 1.0 / total
        prob, low, grad = softmax_grad(expo, dp, [inv] * 3, mixed * inv)
        low = stack(low)
        dq_ref[:, hs] = dot(low, k, 0, 0).astype(BF16)
        for i, out in enumerate((dot(low, q[BLK:], 1, 0), dot(stack(prob), g[BLK:], 1, 0))):
            part_ref[i, :BLK, hs] = out[:BLK]
            part_ref[i, BLK:, hs] = out[BLK:] + mid_in[i, :, hs]
        pay_ref[2 * h : 2 * h + 2, :] = skew_sum(*grad) + pay_in[2 * h : 2 * h + 2, :]
        scores = [s * (SCALE * LOG2E) + t for s, t in zip(cut(raw[: 2 * BLK, :BLK]), [veiled[1], table[2]])]
        dp = cut(dps[: 2 * BLK, :BLK])
        expo, peak, total, mixed = weights(scores, dp)
        for i in range(2):
            expo_ref[2 * h + i] = expo[i]
            dp_ref[2 * h + i] = dp[i]
        for i, x in enumerate((peak, total, mixed)):
            stat_ref[3 * h + i : 3 * h + i + 1, :] = x


def far_body(
    q_ref, g_ref, far_ref, tab_ref, pay_in, expo_ref, dp_ref, stat_ref, pay_ref, prob_ref, low_ref
):
    hidden = hidden_keys()
    pay = []
    for h in range(HEADS):
        hs = head(h)
        score = dot(far_ref[0, :, hs], q_ref[:BLK, hs], 1, 1) * (SCALE * LOG2E) + (tab_ref[3 * h] + hidden)
        dp = dot(far_ref[1, :, hs], g_ref[:BLK, hs], 1, 1)
        peak, total, mixed = (stat_ref[3 * h + i : 3 * h + i + 1, :] for i in range(3))
        top = jnp.maximum(peak, score.max(axis=0, keepdims=True))
        expo = jnp.exp2(score - top)
        fade = jnp.exp2(peak - top)
        inv = 1.0 / (total * fade + sum_of([expo]))
        delta = (mixed * fade + sum_of([expo * dp])) * inv
        fade = fade * inv
        expos = [expo, expo_ref[2 * h], expo_ref[2 * h + 1]]
        dps = [dp, dp_ref[2 * h], dp_ref[2 * h + 1]]
        prob, low, grad = softmax_grad(expos, dps, [inv, fade, fade], delta)
        pay.append(skew_sum(*grad))
        for m in range(3):
            prob_ref[h, m * BLK : (m + 1) * BLK, :] = prob[m]
            low_ref[h, m * BLK : (m + 1) * BLK, :] = low[m]
    total = jnp.concatenate(pay, axis=0) + pay_in[...]
    pay_ref[...] = jnp.broadcast_to(total[None], pay_ref.shape)


def back_body(q_ref, g_ref, part_ref, prob_ref, low_ref, back_ref):
    for h in range(HEADS):
        hs = head(h)
        for i, (w, x) in enumerate(((low_ref, q_ref), (prob_ref, g_ref))):
            out = dot(w[h, : 2 * BLK, :], x[:BLK, hs], 1, 0)
            back_ref[i, :BLK, hs] = out[:BLK].astype(BF16)
            back_ref[i, BLK:, hs] = (out[BLK:] + part_ref[i, :BLK, hs]).astype(BF16)


def join_body(
    q_ref, k_ref, g_ref, near_ref, far_ref, part_ref, end_ref, prob_ref, low_ref, dq1_ref, dq2_ref, back_ref,
    dq_ref, dk_ref, dv_ref,
):
    dq_ref[BLK : 2 * BLK, :] = dq1_ref[...]
    dq_ref[2 * BLK :, :] = dq2_ref[...]
    for i, out in enumerate((dk_ref, dv_ref)):
        out[BLK : 2 * BLK, :] = (part_ref[i, 2 * BLK :, :] + back_ref[i, :BLK, :].astype(F32)).astype(BF16)
        out[2 * BLK :, :] = (end_ref[i] + back_ref[i, BLK:, :].astype(F32)).astype(BF16)
    for h in range(HEADS):
        hs = head(h)
        keys = stack([far_ref[0, :, hs], near_ref[0, :, hs], k_ref[:BLK, hs]])
        dq_ref[:BLK, hs] = dot(low_ref[h], keys, 0, 0).astype(BF16)
        for i, (out, w, x) in enumerate(((dk_ref, low_ref, q_ref), (dv_ref, prob_ref, g_ref))):
            own = dot(w[h, 2 * BLK :, :], x[:BLK, hs], 1, 0)
            out[:BLK, hs] = (own + part_ref[i, BLK : 2 * BLK, hs]).astype(BF16)


def table_body(order, x_ref, o_ref, sum_ref):
    heads = o_ref.shape[0]
    total = jnp.sum(x_ref[...], axis=0)
    span = total.shape[0] // len(order)
    for i, at in enumerate(order):
        sum_ref[at * span : (at + 1) * span, :] = total[i * span : (i + 1) * span]
    low = sum_ref[pl.ds(0, heads, stride=2), :]
    mid = sum_ref[pl.ds(1, heads, stride=2), :]
    lane = lax.broadcasted_iota(jnp.int32, low.shape, 1)
    top = jnp.sum(jnp.where(lane < SEG, low, 0.0), axis=1, keepdims=True)
    mid = pltpu.roll(mid, SEG - 1, 1)
    first = jnp.where(lane < SEG - 1, pltpu.roll(low, SEG - 1, 1), mid)
    last = jnp.where(lane < SEG - 1, mid, top)
    o_ref[:, :BLK] = first
    o_ref[:, BLK:] = last[:, : BUCKETS - BLK]


def call(body, name, outs, args, spaces=None, scratch=(), mib=8):
    return pl.pallas_call(
        body,
        out_shape=tuple(jax.ShapeDtypeStruct(*o) for o in outs),
        in_specs=spaces or [VMEM] * len(args),
        out_specs=(VMEM,) * len(outs),
        scratch_shapes=scratch,
        compiler_params=pltpu.CompilerParams(vmem_limit_bytes=mib << 20),
        name=name,
    )(*args)


def ordered(count, first):
    return [(first + i) % count for i in range(count)]


def exchange(x, size, outer, inner):
    rest = [a for a in AXES if a not in (outer[0], inner[0])]
    step = {a: math.prod(size[b] for b in AXES[AXES.index(a) + 1 :]) for a in AXES}
    groups = [
        [i * step[rest[0]] + j * step[rest[1]] + m * step[outer[0]] + n * step[inner[0]] for m in outer[1] for n in inner[1]]
        for i in range(size[rest[0]])
        for j in range(size[rest[1]])
    ]
    return lax.all_to_all(x, AXES, split_axis=0, concat_axis=0, axis_index_groups=groups, tiled=True)


def local(queries, keys, values, rel_bias, out_grad):
    _, rows, width = queries.shape
    q, k, v, g = (a.reshape(rows, width) for a in (queries, keys, values, out_grad))
    size = {a: lax.axis_size(a) for a in AXES}
    count = size["z"] * size["y"]
    pair = (2, BLK, width)
    kept = tuple(pltpu.with_memory_space_constraint(a, pltpu.HBM) for a in (k, v))
    near, far = call(
        tails_body, "tails", [(pair, BF16)] * 2, kept, [HBM] * 2, [pltpu.SemaphoreType.DMA((4,))], 4
    )
    ahead = [(s, s + 1) for s in range(count - 1)]
    near = lax.ppermute(near, ("z", "y"), ahead)
    far = lax.ppermute(far, ("z", "y"), ahead)
    dq2, mid, end, pay, table = call(
        own_body,
        "own",
        [
            ((BLK, width), BF16),
            ((2, 2 * BLK, width), F32),
            (pair, F32),
            ((2 * HEADS, BLK), F32),
            ((3 * HEADS, BLK, BLK), F32),
        ],
        (q, k, v, g, rel_bias),
        scratch=[pltpu.VMEM((8, 2 * BLK), F32)],
    )
    dq1, part, pay, expo, dp, stat = call(
        near_body,
        "near",
        [
            ((BLK, width), BF16),
            ((2, 3 * BLK, width), F32),
            ((2 * HEADS, BLK), F32),
            ((2 * HEADS, BLK, BLK), F32),
            ((2 * HEADS, BLK, BLK), F32),
            ((8, BLK), F32),
        ],
        (q, k, v, g, near, table, mid, pay),
    )
    group = size["y"] * size["c"]
    z_order, y_order, x_order = ordered(size["z"], 7), ordered(size["y"], 4), ordered(size["x"], 2)
    pay, prob, low = call(
        far_body,
        "far",
        [
            ((group, 2 * HEADS, BLK), F32),
            ((HEADS, 3 * BLK, BLK), BF16),
            ((HEADS, 3 * BLK, BLK), BF16),
        ],
        (q, g, far, table, pay, expo, dp, stat),
    )
    pay = exchange(pay, size, ("y", y_order), ("c", range(size["c"])))
    (back,) = call(back_body, "back", [((2, 2 * BLK, width), BF16)], (q, g, part, prob, low))
    back = lax.ppermute(back, ("z", "y"), [(s + 1, s) for s in range(count - 1)])
    pay = pay.reshape(size["y"], size["c"] * 2 * HEADS, BLK).sum(axis=0)
    pay = jnp.broadcast_to(pay, (size["z"] * size["x"], *pay.shape))
    pay = exchange(pay, size, ("z", z_order), ("x", x_order))
    dq, dk, dv = call(
        join_body,
        "join",
        [((rows, width), BF16)] * 3,
        (q, k, g, near, far, part, end, prob, low, dq1, dq2, back),
    )
    (bias,) = call(
        functools.partial(table_body, x_order),
        "table",
        [((size["x"] * size["c"] * HEADS, BUCKETS), F32)],
        (pay.reshape(size["z"], size["x"] * size["c"] * 2 * HEADS, BLK),),
        scratch=[pltpu.VMEM((size["x"] * size["c"] * 2 * HEADS, BLK), F32)],
        mib=4,
    )
    return tuple(a.reshape(queries.shape) for a in (dq, dk, dv)) + (bias,)


def solution(mesh):
    sp, tp = mesh.devices.shape
    split = Mesh(mesh.devices.reshape(8, sp // 8, tp // 2, 2), AXES)
    rows = P(None, ("z", "y"), ("x", "c"))
    return jax.shard_map(
        local,
        mesh=split,
        in_specs=(rows, rows, rows, P(("x", "c"), None), rows),
        out_specs=(rows, rows, rows, P()),
        check_vma=False,
    )
```

```python
import functools
import math

import jax
import jax.numpy as jnp
from jax import lax
from jax.experimental import pallas as pl
from jax.experimental.pallas import tpu as pltpu
from jax.sharding import Mesh, PartitionSpec as P

HEAD_DIM = 128
SEG = 64
LEFT = 4
CLIP = 128
BUCKETS = 192
HEADS = 2
BLK = 128
SCALE = HEAD_DIM**-0.5
LOG2E = 1.4426950408889634
NEG = -1e30
F32 = jnp.float32
BF16 = jnp.bfloat16
VMEM = pl.BlockSpec(memory_space=pltpu.VMEM)
HBM = pl.BlockSpec(memory_space=pltpu.HBM)
AXES = ("z", "y", "x", "c")


def dot(a, b, ca, cb):
    return lax.dot_general(a, b, (((ca,), (cb,)), ((), ())), preferred_element_type=F32)


def iotas():
    c = lax.broadcasted_iota(jnp.int32, (BLK, BLK), 0)
    r = lax.broadcasted_iota(jnp.int32, (BLK, BLK), 1)
    return c, r


def bias_blocks(row):
    c, r = iotas()
    row = row * LOG2E
    wide = jnp.broadcast_to(row, (8, 2 * BLK))
    mid = pltpu.roll(wide, 2 * BLK - (SEG - 1), 1)[:1, :BLK]
    low = pltpu.roll(wide, SEG + 1, 1)[:1, :BLK]
    top = wide[:1, BUCKETS - 1 : BUCKETS]
    mid = pltpu.roll(jnp.broadcast_to(mid, (BLK, BLK)), 0, 1, stride=1, stride_axis=0)
    low = pltpu.roll(jnp.broadcast_to(low, (BLK, BLK)), 0, 1, stride=1, stride_axis=0)
    t0 = jnp.where((c < SEG) & (r >= SEG), NEG, top)
    t1 = jnp.where(r >= c, top, mid)
    t2 = jnp.where(r >= c, mid, jnp.where((c >= SEG) & (r < SEG), NEG, low))
    return t0, t1, t2


def along_diagonals(x):
    acc = x[:8]
    for a in range(8, BLK, 8):
        acc = acc + pltpu.roll(x[a : a + 8], BLK - a, 1)
    row = lax.broadcasted_iota(jnp.int32, acc.shape, 0)
    out = acc
    for b in range(1, 8):
        out = jnp.where(row == b, pltpu.roll(acc, BLK - b, 1), out)
    return jnp.sum(out, axis=0, keepdims=True)


def skew_sum(d0, d1, d2):
    c, r = iotas()
    upper = r >= c
    mid = along_diagonals(jnp.where(upper, d2, d1))
    low = along_diagonals(jnp.where(upper, 0.0, d2))
    top = jnp.sum(jnp.where(upper, d1, 0.0) + d0, axis=0, keepdims=True)
    top = top + pltpu.roll(jnp.broadcast_to(top, (8, BLK)), SEG, 1)[:1]
    low = jnp.where(r[:1] < SEG, top, low)
    return jnp.concatenate([low, mid], axis=0)


def softmax_grad(expo, prob_grads, inv, delta):
    prob = [e * i for e, i in zip(expo, inv)]
    grad = [p * (g - delta) for p, g in zip(prob, prob_grads)]
    return [p.astype(BF16) for p in prob], [(g * SCALE).astype(BF16) for g in grad], grad


def peak_of(scores):
    return functools.reduce(jnp.maximum, scores).max(axis=0, keepdims=True)


def sum_of(blocks):
    return functools.reduce(jnp.add, blocks).sum(axis=0, keepdims=True)


def sum_rows(x):
    return x.sum(axis=0, keepdims=True)


def weights(scores, prob_grads):
    peak = peak_of(scores)
    expo = [jnp.exp2(s - peak) for s in scores]
    return expo, peak, sum_of(expo), sum_of([e * g for e, g in zip(expo, prob_grads)])


def cut(x):
    return [x[at : at + BLK] for at in range(0, x.shape[0], BLK)]


def stack(blocks):
    return jnp.concatenate(blocks, axis=0)


def head(h):
    return slice(h * HEAD_DIM, (h + 1) * HEAD_DIM)


def hidden_keys():
    first = (lax.axis_index("z") == 0) & (lax.axis_index("y") == 0)
    return jnp.where(first, NEG, 0.0).astype(F32)


def start_all(copies):
    for copy in copies:
        copy.start()
    return copies


def wait_all(copies):
    for copy in copies:
        copy.wait()


def tails_body(k_ref, v_ref, near_ref, far_ref, sem):
    first = k_ref.shape[0] - near_ref.shape[1] - far_ref.shape[1]
    copies = [
        pltpu.make_async_copy(ref.at[pl.ds(first + at, out.shape[1])], out.at[i], sem.at[2 * i + j])
        for i, ref in enumerate((k_ref, v_ref))
        for j, (out, at) in enumerate(((near_ref, far_ref.shape[1]), (far_ref, 0)))
    ]
    wait_all(start_all(copies))


def own_body(
    q_hbm, k_hbm, v_hbm, g_hbm, rb_ref,
    q_ref, k_ref, v_ref, g_ref, dq_ref, mid_ref, end_ref, pay_ref, tab_ref, rb_pad, sem,
):
    loads = ((k_hbm, k_ref), (q_hbm, q_ref), (v_hbm, v_ref), (g_hbm, g_ref))
    loads = start_all([pltpu.make_async_copy(x, y, sem.at[i]) for i, (x, y) in enumerate(loads)])
    rb_pad[...] = jnp.zeros_like(rb_pad)
    rb_pad[0:HEADS, 0:BUCKETS] = rb_ref[...]
    for h in range(HEADS):
        for m, block in enumerate(bias_blocks(rb_pad[h : h + 1, :])):
            tab_ref[3 * h + m] = block
    wait_all(loads)
    for h in range(HEADS):
        hs = head(h)
        table = [tab_ref[3 * h + m] for m in range(3)]
        k = k_ref[:, hs]
        q = q_ref[2 * BLK :, hs]
        g = g_ref[2 * BLK :, hs]
        scores = [s * (SCALE * LOG2E) + t for s, t in zip(cut(dot(k, q, 1, 1)), table)]
        dp = cut(dot(v_ref[:, hs], g, 1, 1))
        expo, _, total, mixed = weights(scores, dp)
        inv = 1.0 / total
        prob, low, grad = softmax_grad(expo, dp, [inv] * 3, mixed * inv)
        low = stack(low)
        dq_ref[:, hs] = dot(low, k, 0, 0).astype(BF16)
        for i, out in enumerate((dot(low, q, 1, 0), dot(stack(prob), g, 1, 0))):
            mid_ref[i, :, hs] = out[: 2 * BLK]
            end_ref[i, :, hs] = out[2 * BLK :]
        pay_ref[2 * h : 2 * h + 2, :] = skew_sum(*grad)


def near_body(
    q_ref, k_ref, v_ref, g_ref, near_ref, tab_ref, mid_in, pay_in,
    dq_ref, part_ref, pay_ref, expo_ref, dp_ref, stat_ref,
):
    hidden = hidden_keys()
    for h in range(HEADS):
        hs = head(h)
        table = [tab_ref[3 * h + m] for m in range(3)]
        k = stack([near_ref[0, :, hs], k_ref[: 2 * BLK, hs]])
        v = stack([near_ref[1, :, hs], v_ref[: 2 * BLK, hs]])
        q = q_ref[: 2 * BLK, hs]
        g = g_ref[: 2 * BLK, hs]
        raw = dot(k, q, 1, 1)
        dps = dot(v, g, 1, 1)
        scores = [s * (SCALE * LOG2E) + t for s, t in zip(cut(raw[SEG:, BLK:]), [table[0] + hidden] + table[1:])]
        dp = cut(dps[SEG:, BLK:])
        expo, _, total, mixed = weights(scores, dp)
        inv = 1.0 / total
        prob, low, grad = softmax_grad(expo, dp, [inv] * 3, mixed * inv)
        low = stack(low)
        dq_ref[:, hs] = dot(low, k[SEG:], 0, 0).astype(BF16)
        for i, out in enumerate((dot(low, q[BLK:], 1, 0), dot(stack(prob), g[BLK:], 1, 0))):
            part_ref[i, :BLK, hs] = out[:BLK]
            part_ref[i, BLK:, hs] = out[BLK:] + mid_in[i, :, hs]
        pay_ref[2 * h : 2 * h + 2, :] = skew_sum(*grad) + pay_in[2 * h : 2 * h + 2, :]
        shift = stack([table[0][SEG:] + hidden, table[1] + hidden, table[2]])
        rows = shift.shape[0]
        score = raw[:rows, :BLK] * (SCALE * LOG2E) + shift
        dp = dps[:rows, :BLK]
        peak = score.max(axis=0, keepdims=True)
        expo = jnp.exp2(score - peak)
        expo_ref[h] = expo
        dp_ref[h] = dp
        for i, x in enumerate((peak, sum_rows(expo), sum_rows(expo * dp))):
            stat_ref[3 * h + i : 3 * h + i + 1, :] = x


def far_body(
    q_ref, g_ref, far_ref, tab_ref, pay_in, expo_ref, dp_ref, stat_ref, pay_ref, prob_ref, low_ref
):
    hidden = hidden_keys()
    pay = []
    for h in range(HEADS):
        hs = head(h)
        score = dot(far_ref[0, :, hs], q_ref[:BLK, hs], 1, 1) * (SCALE * LOG2E) + (tab_ref[3 * h, :SEG, :] + hidden)
        dp = dot(far_ref[1, :, hs], g_ref[:BLK, hs], 1, 1)
        peak, total, mixed = (stat_ref[3 * h + i : 3 * h + i + 1, :] for i in range(3))
        top = jnp.maximum(peak, score.max(axis=0, keepdims=True))
        expo = jnp.exp2(score - top)
        fade = jnp.exp2(peak - top)
        inv = 1.0 / (total * fade + sum_rows(expo))
        delta = (mixed * fade + sum_rows(expo * dp)) * inv
        prob = stack([expo * inv, expo_ref[h] * (fade * inv)])
        grad = prob * (stack([dp, dp_ref[h]]) - delta)
        prob_ref[h] = prob.astype(BF16)
        low_ref[h] = (grad * SCALE).astype(BF16)
        pay.append(skew_sum(*cut(grad)))
    total = jnp.concatenate(pay, axis=0) + pay_in[...]
    pay_ref[...] = jnp.broadcast_to(total[None], pay_ref.shape)


def back_body(q_ref, g_ref, part_ref, prob_ref, low_ref, back_ref):
    for h in range(HEADS):
        hs = head(h)
        for i, (w, x) in enumerate(((low_ref, q_ref), (prob_ref, g_ref))):
            out = dot(w[h, : 2 * BLK, :], x[:BLK, hs], 1, 0)
            back_ref[i, :BLK, hs] = out[:BLK].astype(BF16)
            back_ref[i, BLK:, hs] = (out[BLK:] + part_ref[i, :BLK, hs]).astype(BF16)


def join_body(
    q_ref, k_ref, g_ref, near_ref, far_ref, part_ref, end_ref, prob_ref, low_ref, dq1_ref, dq2_ref, back_ref,
    dq_ref, dk_ref, dv_ref,
):
    dq_ref[BLK : 2 * BLK, :] = dq1_ref[...]
    dq_ref[2 * BLK :, :] = dq2_ref[...]
    for i, out in enumerate((dk_ref, dv_ref)):
        out[BLK : 2 * BLK, :] = (part_ref[i, 2 * BLK :, :] + back_ref[i, :BLK, :].astype(F32)).astype(BF16)
        out[2 * BLK :, :] = (end_ref[i] + back_ref[i, BLK:, :].astype(F32)).astype(BF16)
    for h in range(HEADS):
        hs = head(h)
        keys = stack([far_ref[0, :, hs], near_ref[0, :, hs], k_ref[:BLK, hs]])
        dq_ref[:BLK, hs] = dot(low_ref[h], keys, 0, 0).astype(BF16)
        for i, (out, w, x) in enumerate(((dk_ref, low_ref, q_ref), (dv_ref, prob_ref, g_ref))):
            own = dot(w[h, 2 * BLK :, :], x[:BLK, hs], 1, 0)
            out[:BLK, hs] = (own + part_ref[i, BLK : 2 * BLK, hs]).astype(BF16)


def table_body(order, x_ref, o_ref, sum_ref):
    heads = o_ref.shape[0]
    total = jnp.sum(x_ref[...], axis=0)
    span = total.shape[0] // len(order)
    for i, at in enumerate(order):
        sum_ref[at * span : (at + 1) * span, :] = total[i * span : (i + 1) * span]
    low = sum_ref[pl.ds(0, heads, stride=2), :]
    mid = sum_ref[pl.ds(1, heads, stride=2), :]
    lane = lax.broadcasted_iota(jnp.int32, low.shape, 1)
    top = jnp.sum(jnp.where(lane < SEG, low, 0.0), axis=1, keepdims=True)
    mid = pltpu.roll(mid, SEG - 1, 1)
    first = jnp.where(lane < SEG - 1, pltpu.roll(low, SEG - 1, 1), mid)
    last = jnp.where(lane < SEG - 1, mid, top)
    o_ref[:, :BLK] = first
    o_ref[:, BLK:] = last[:, : BUCKETS - BLK]


def call(body, name, outs, args, spaces=None, scratch=(), mib=8):
    return pl.pallas_call(
        body,
        out_shape=tuple(jax.ShapeDtypeStruct(*o) for o in outs),
        in_specs=spaces or [VMEM] * len(args),
        out_specs=(VMEM,) * len(outs),
        scratch_shapes=scratch,
        compiler_params=pltpu.CompilerParams(vmem_limit_bytes=mib << 20),
        name=name,
    )(*args)


def ordered(count, first):
    return [(first + i) % count for i in range(count)]


def exchange(x, size, outer, inner):
    rest = [a for a in AXES if a not in (outer[0], inner[0])]
    step = {a: math.prod(size[b] for b in AXES[AXES.index(a) + 1 :]) for a in AXES}
    groups = [
        [i * step[rest[0]] + j * step[rest[1]] + m * step[outer[0]] + n * step[inner[0]] for m in outer[1] for n in inner[1]]
        for i in range(size[rest[0]])
        for j in range(size[rest[1]])
    ]
    return lax.all_to_all(x, AXES, split_axis=0, concat_axis=0, axis_index_groups=groups, tiled=True)


def local(queries, keys, values, rel_bias, out_grad):
    _, rows, width = queries.shape
    q, k, v, g = (a.reshape(rows, width) for a in (queries, keys, values, out_grad))
    size = {a: lax.axis_size(a) for a in AXES}
    count = size["z"] * size["y"]
    pair = (2, BLK, width)
    q, k, v, g = (pltpu.with_memory_space_constraint(a, pltpu.HBM) for a in (q, k, v, g))
    near, far = call(
        tails_body,
        "tails",
        [((2, LEFT * SEG - SEG, width), BF16), ((2, SEG, width), BF16)],
        (k, v),
        [HBM] * 2,
        [pltpu.SemaphoreType.DMA((4,))],
        4,
    )
    ahead = [(s, s + 1) for s in range(count - 1)]
    near = lax.ppermute(near, ("z", "y"), ahead)
    far = lax.ppermute(far, ("z", "y"), ahead)
    q, k, v, g, dq2, mid, end, pay, table = call(
        own_body,
        "own",
        [((rows, width), BF16)] * 4
        + [
            ((BLK, width), BF16),
            ((2, 2 * BLK, width), F32),
            (pair, F32),
            ((2 * HEADS, BLK), F32),
            ((3 * HEADS, BLK, BLK), F32),
        ],
        (q, k, v, g, rel_bias),
        [HBM] * 4 + [VMEM],
        [pltpu.VMEM((8, 2 * BLK), F32), pltpu.SemaphoreType.DMA((4,))],
    )
    seen = (HEADS, 2 * BLK + SEG, BLK)
    dq1, part, pay, expo, dp, stat = call(
        near_body,
        "near",
        [
            ((BLK, width), BF16),
            ((2, 3 * BLK, width), F32),
            ((2 * HEADS, BLK), F32),
            (seen, F32),
            (seen, F32),
            ((8, BLK), F32),
        ],
        (q, k, v, g, near, table, mid, pay),
    )
    group = size["y"] * size["c"]
    z_order, y_order, x_order = [5,0,1,7,2,6,3,4], ordered(size["y"], 4), ordered(size["x"], 2)
    pay, prob, low = call(
        far_body,
        "far",
        [
            ((group, 2 * HEADS, BLK), F32),
            ((HEADS, 3 * BLK, BLK), BF16),
            ((HEADS, 3 * BLK, BLK), BF16),
        ],
        (q, g, far, table, pay, expo, dp, stat),
    )
    pay = exchange(pay, size, ("y", y_order), ("c", range(size["c"])))
    (back,) = call(back_body, "back", [((2, 2 * BLK, width), BF16)], (q, g, part, prob, low))
    back = lax.ppermute(back, ("z", "y"), [(s + 1, s) for s in range(count - 1)])
    pay = pay.reshape(size["y"], size["c"] * 2 * HEADS, BLK).sum(axis=0)
    pay = jnp.broadcast_to(pay, (size["z"] * size["x"], *pay.shape))
    pay = exchange(pay, size, ("z", z_order), ("x", x_order))
    dq, dk, dv = call(
        join_body,
        "join",
        [((rows, width), BF16)] * 3,
        (q, k, g, near, far, part, end, prob, low, dq1, dq2, back),
    )
    (bias,) = call(
        functools.partial(table_body, x_order),
        "table",
        [((size["x"] * size["c"] * HEADS, BUCKETS), F32)],
        (pay.reshape(size["z"], size["x"] * size["c"] * 2 * HEADS, BLK),),
        scratch=[pltpu.VMEM((size["x"] * size["c"] * 2 * HEADS, BLK), F32)],
        mib=4,
    )
    return tuple(a.reshape(queries.shape) for a in (dq, dk, dv)) + (bias,)


def solution(mesh):
    sp, tp = mesh.devices.shape
    split = Mesh(mesh.devices.reshape(8, sp // 8, tp // 2, 2), AXES)
    rows = P(None, ("z", "y"), ("x", "c"))
    return jax.shard_map(
        local,
        mesh=split,
        in_specs=(rows, rows, rows, P(("x", "c"), None), rows),
        out_specs=(rows, rows, rows, P()),
        check_vma=False,
    )
```

```python
import functools
import math

import jax
import jax.numpy as jnp
from jax import lax
from jax.experimental import pallas as pl
from jax.experimental.pallas import tpu as pltpu
from jax.sharding import Mesh, PartitionSpec as P

HEAD_DIM = 128
SEG = 64
LEFT = 4
CLIP = 128
BUCKETS = 192
HEADS = 2
BLK = 128
SCALE = HEAD_DIM**-0.5
LOG2E = 1.4426950408889634
NEG = -1e30
F32 = jnp.float32
BF16 = jnp.bfloat16
VMEM = pl.BlockSpec(memory_space=pltpu.VMEM)
HBM = pl.BlockSpec(memory_space=pltpu.HBM)
AXES = ("z", "y", "x", "c")
ORDERS = {"z": (5, 3, 2, 1, 0, 4, 7, 6), "y": (4, 5, 3, 6, 2, 7, 1, 0), "x": (2, 1, 3, 0), "c": (1, 0)}


def dot(a, b, ca, cb):
    return lax.dot_general(a, b, (((ca,), (cb,)), ((), ())), preferred_element_type=F32)


def iotas():
    c = lax.broadcasted_iota(jnp.int32, (BLK, BLK), 0)
    r = lax.broadcasted_iota(jnp.int32, (BLK, BLK), 1)
    return c, r


def bias_blocks(row):
    c, r = iotas()
    row = row * LOG2E
    wide = jnp.broadcast_to(row, (8, 2 * BLK))
    mid = pltpu.roll(wide, 2 * BLK - (SEG - 1), 1)[:1, :BLK]
    low = pltpu.roll(wide, SEG + 1, 1)[:1, :BLK]
    top = wide[:1, BUCKETS - 1 : BUCKETS]
    mid = pltpu.roll(jnp.broadcast_to(mid, (BLK, BLK)), 0, 1, stride=1, stride_axis=0)
    low = pltpu.roll(jnp.broadcast_to(low, (BLK, BLK)), 0, 1, stride=1, stride_axis=0)
    t0 = jnp.where((c < SEG) & (r >= SEG), NEG, top)
    t1 = jnp.where(r >= c, top, mid)
    t2 = jnp.where(r >= c, mid, jnp.where((c >= SEG) & (r < SEG), NEG, low))
    return t0, t1, t2


def along_diagonals(x):
    acc = x[:8]
    for a in range(8, BLK, 8):
        acc = acc + pltpu.roll(x[a : a + 8], BLK - a, 1)
    row = lax.broadcasted_iota(jnp.int32, acc.shape, 0)
    out = acc
    for b in range(1, 8):
        out = jnp.where(row == b, pltpu.roll(acc, BLK - b, 1), out)
    return jnp.sum(out, axis=0, keepdims=True)


def skew_sum(d0, d1, d2):
    c, r = iotas()
    upper = r >= c
    mid = along_diagonals(jnp.where(upper, d2, d1))
    low = along_diagonals(jnp.where(upper, 0.0, d2))
    top = jnp.sum(jnp.where(upper, d1, 0.0) + d0, axis=0, keepdims=True)
    top = top + pltpu.roll(jnp.broadcast_to(top, (8, BLK)), SEG, 1)[:1]
    low = jnp.where(r[:1] < SEG, top, low)
    return jnp.concatenate([low, mid], axis=0)


def softmax_grad(expo, prob_grads, inv, delta):
    prob = [e * i for e, i in zip(expo, inv)]
    grad = [p * (g - delta) for p, g in zip(prob, prob_grads)]
    return [p.astype(BF16) for p in prob], [(g * SCALE).astype(BF16) for g in grad], grad


def peak_of(scores):
    return functools.reduce(jnp.maximum, scores).max(axis=0, keepdims=True)


def sum_of(blocks):
    return functools.reduce(jnp.add, blocks).sum(axis=0, keepdims=True)


def sum_rows(x):
    return x.sum(axis=0, keepdims=True)


def weights(scores, prob_grads):
    peak = peak_of(scores)
    expo = [jnp.exp2(s - peak) for s in scores]
    return expo, peak, sum_of(expo), sum_of([e * g for e, g in zip(expo, prob_grads)])


def cut(x):
    return [x[at : at + BLK] for at in range(0, x.shape[0], BLK)]


def stack(blocks):
    return jnp.concatenate(blocks, axis=0)


def head(h):
    return slice(h * HEAD_DIM, (h + 1) * HEAD_DIM)


def hidden_keys():
    first = (lax.axis_index("z") == 0) & (lax.axis_index("y") == 0)
    return jnp.where(first, NEG, 0.0).astype(F32)


def start_all(copies):
    for copy in copies:
        copy.start()
    return copies


def wait_all(copies):
    for copy in copies:
        copy.wait()


def tails_body(k_ref, v_ref, near_ref, far_ref, sem):
    first = k_ref.shape[0] - near_ref.shape[1] - far_ref.shape[1]
    copies = [
        pltpu.make_async_copy(ref.at[pl.ds(first + at, out.shape[1])], out.at[i], sem.at[2 * i + j])
        for i, ref in enumerate((k_ref, v_ref))
        for j, (out, at) in enumerate(((near_ref, far_ref.shape[1]), (far_ref, 0)))
    ]
    wait_all(start_all(copies))


def own_body(
    q_hbm, k_hbm, v_hbm, g_hbm, rb_ref,
    q_ref, k_ref, v_ref, g_ref, dq_ref, mid_ref, end_ref, pay_ref, tab_ref, rb_pad, sem,
):
    loads = ((k_hbm, k_ref), (q_hbm, q_ref), (v_hbm, v_ref), (g_hbm, g_ref))
    loads = start_all([pltpu.make_async_copy(x, y, sem.at[i]) for i, (x, y) in enumerate(loads)])
    rb_pad[...] = jnp.zeros_like(rb_pad)
    rb_pad[0:HEADS, 0:BUCKETS] = rb_ref[...]
    for h in range(HEADS):
        for m, block in enumerate(bias_blocks(rb_pad[h : h + 1, :])):
            tab_ref[3 * h + m] = block
    wait_all(loads)
    for h in range(HEADS):
        hs = head(h)
        table = [tab_ref[3 * h + m] for m in range(3)]
        k = k_ref[:, hs]
        q = q_ref[2 * BLK :, hs]
        g = g_ref[2 * BLK :, hs]
        scores = [s * (SCALE * LOG2E) + t for s, t in zip(cut(dot(k, q, 1, 1)), table)]
        dp = cut(dot(v_ref[:, hs], g, 1, 1))
        expo, _, total, mixed = weights(scores, dp)
        inv = 1.0 / total
        prob, low, grad = softmax_grad(expo, dp, [inv] * 3, mixed * inv)
        low = stack(low)
        dq_ref[:, hs] = dot(low, k, 0, 0).astype(BF16)
        for i, out in enumerate((dot(low, q, 1, 0), dot(stack(prob), g, 1, 0))):
            mid_ref[i, :, hs] = out[: 2 * BLK]
            end_ref[i, :, hs] = out[2 * BLK :]
        pay_ref[2 * h : 2 * h + 2, :] = skew_sum(*grad)


def near_body(
    q_ref, k_ref, v_ref, g_ref, near_ref, tab_ref, mid_in, pay_in,
    dq_ref, part_ref, pay_ref, expo_ref, dp_ref, stat_ref,
):
    hidden = hidden_keys()
    for h in range(HEADS):
        hs = head(h)
        table = [tab_ref[3 * h + m] for m in range(3)]
        k = stack([near_ref[0, :, hs], k_ref[: 2 * BLK, hs]])
        v = stack([near_ref[1, :, hs], v_ref[: 2 * BLK, hs]])
        q = q_ref[: 2 * BLK, hs]
        g = g_ref[: 2 * BLK, hs]
        raw = dot(k, q, 1, 1)
        dps = dot(v, g, 1, 1)
        scores = [s * (SCALE * LOG2E) + t for s, t in zip(cut(raw[SEG:, BLK:]), [table[0] + hidden] + table[1:])]
        dp = cut(dps[SEG:, BLK:])
        expo, _, total, mixed = weights(scores, dp)
        inv = 1.0 / total
        prob, low, grad = softmax_grad(expo, dp, [inv] * 3, mixed * inv)
        low = stack(low)
        dq_ref[:, hs] = dot(low, k[SEG:], 0, 0).astype(BF16)
        for i, out in enumerate((dot(low, q[BLK:], 1, 0), dot(stack(prob), g[BLK:], 1, 0))):
            part_ref[i, :BLK, hs] = out[:BLK]
            part_ref[i, BLK:, hs] = out[BLK:] + mid_in[i, :, hs]
        pay_ref[2 * h : 2 * h + 2, :] = skew_sum(*grad) + pay_in[2 * h : 2 * h + 2, :]
        shift = stack([table[0][SEG:] + hidden, table[1] + hidden, table[2]])
        rows = shift.shape[0]
        score = raw[:rows, :BLK] * (SCALE * LOG2E) + shift
        dp = dps[:rows, :BLK]
        peak = score.max(axis=0, keepdims=True)
        expo = jnp.exp2(score - peak)
        expo_ref[h] = expo
        dp_ref[h] = dp
        for i, x in enumerate((peak, sum_rows(expo), sum_rows(expo * dp))):
            stat_ref[3 * h + i : 3 * h + i + 1, :] = x


def far_body(
    q_ref, g_ref, far_ref, tab_ref, pay_in, expo_ref, dp_ref, stat_ref, part_ref,
    pay_hbm, prob_ref, low_ref, back_ref, pay_ref, sem,
):
    hidden = hidden_keys()
    pay = []
    for h in range(HEADS):
        hs = head(h)
        score = dot(far_ref[0, :, hs], q_ref[:BLK, hs], 1, 1) * (SCALE * LOG2E) + (tab_ref[3 * h, :SEG, :] + hidden)
        dp = dot(far_ref[1, :, hs], g_ref[:BLK, hs], 1, 1)
        peak, total, mixed = (stat_ref[3 * h + i : 3 * h + i + 1, :] for i in range(3))
        top = jnp.maximum(peak, score.max(axis=0, keepdims=True))
        expo = jnp.exp2(score - top)
        fade = jnp.exp2(peak - top)
        inv = 1.0 / (total * fade + sum_rows(expo))
        delta = (mixed * fade + sum_rows(expo * dp)) * inv
        prob = stack([expo * inv, expo_ref[h] * (fade * inv)])
        grad = prob * (stack([dp, dp_ref[h]]) - delta)
        prob_ref[h] = prob.astype(BF16)
        low_ref[h] = (grad * SCALE).astype(BF16)
        pay.append(skew_sum(*cut(grad)))
    total = jnp.concatenate(pay, axis=0) + pay_in[...]
    pay_ref[...] = jnp.broadcast_to(total[None], pay_ref.shape)
    copy = pltpu.make_async_copy(pay_ref, pay_hbm, sem)
    copy.start()
    for h in range(HEADS):
        hs = head(h)
        for i, (w, x) in enumerate(((low_ref, q_ref), (prob_ref, g_ref))):
            out = dot(w[h, : 2 * BLK, :], x[:BLK, hs], 1, 0)
            back_ref[i, :BLK, hs] = out[:BLK].astype(BF16)
            back_ref[i, BLK:, hs] = (out[BLK:] + part_ref[i, :BLK, hs]).astype(BF16)
    copy.wait()


def join_body(
    q_ref, k_ref, g_ref, near_ref, far_ref, part_ref, end_ref, prob_ref, low_ref, dq1_ref, dq2_ref, back_ref,
    dq_ref, dk_ref, dv_ref,
):
    dq_ref[BLK : 2 * BLK, :] = dq1_ref[...]
    dq_ref[2 * BLK :, :] = dq2_ref[...]
    for i, out in enumerate((dk_ref, dv_ref)):
        out[BLK : 2 * BLK, :] = (part_ref[i, 2 * BLK :, :] + back_ref[i, :BLK, :].astype(F32)).astype(BF16)
        out[2 * BLK :, :] = (end_ref[i] + back_ref[i, BLK:, :].astype(F32)).astype(BF16)
    for h in range(HEADS):
        hs = head(h)
        keys = stack([far_ref[0, :, hs], near_ref[0, :, hs], k_ref[:BLK, hs]])
        dq_ref[:BLK, hs] = dot(low_ref[h], keys, 0, 0).astype(BF16)
        for i, (out, w, x) in enumerate(((dk_ref, low_ref, q_ref), (dv_ref, prob_ref, g_ref))):
            own = dot(w[h, 2 * BLK :, :], x[:BLK, hs], 1, 0)
            out[:BLK, hs] = (own + part_ref[i, BLK : 2 * BLK, hs]).astype(BF16)


def table_body(x_order, c_order, x_ref, o_ref, sum_ref):
    heads = o_ref.shape[0]
    total = jnp.sum(x_ref[...], axis=0)
    cores = len(c_order)
    span = total.shape[0] // (len(x_order) * cores)
    for i, x in enumerate(x_order):
        for j, c in enumerate(c_order):
            at, to = (i * cores + j) * span, (x * cores + c) * span
            sum_ref[to : to + span, :] = total[at : at + span]
    low = sum_ref[pl.ds(0, heads, stride=2), :]
    mid = sum_ref[pl.ds(1, heads, stride=2), :]
    lane = lax.broadcasted_iota(jnp.int32, low.shape, 1)
    top = jnp.sum(jnp.where(lane < SEG, low, 0.0), axis=1, keepdims=True)
    mid = pltpu.roll(mid, SEG - 1, 1)
    first = jnp.where(lane < SEG - 1, pltpu.roll(low, SEG - 1, 1), mid)
    last = jnp.where(lane < SEG - 1, mid, top)
    o_ref[:, :BLK] = first
    o_ref[:, BLK:] = last[:, : BUCKETS - BLK]


def call(body, name, outs, args, spaces=None, scratch=(), mib=8, outputs=None):
    return pl.pallas_call(
        body,
        out_shape=tuple(jax.ShapeDtypeStruct(*o) for o in outs),
        in_specs=spaces or [VMEM] * len(args),
        out_specs=outputs or (VMEM,) * len(outs),
        scratch_shapes=scratch,
        compiler_params=pltpu.CompilerParams(vmem_limit_bytes=mib << 20),
        name=name,
    )(*args)


def late_first(count, order):
    return [i for i in order if i < count] + [i for i in range(count) if i not in order]


def exchange(x, size, outer, inner):
    rest = [a for a in AXES if a not in (outer[0], inner[0])]
    step = {a: math.prod(size[b] for b in AXES[AXES.index(a) + 1 :]) for a in AXES}
    groups = [
        [i * step[rest[0]] + j * step[rest[1]] + m * step[outer[0]] + n * step[inner[0]] for m in outer[1] for n in inner[1]]
        for i in range(size[rest[0]])
        for j in range(size[rest[1]])
    ]
    return lax.all_to_all(x, AXES, split_axis=0, concat_axis=0, axis_index_groups=groups, tiled=True)


def local(queries, keys, values, rel_bias, out_grad):
    _, rows, width = queries.shape
    q, k, v, g = (a.reshape(rows, width) for a in (queries, keys, values, out_grad))
    size = {a: lax.axis_size(a) for a in AXES}
    count = size["z"] * size["y"]
    pair = (2, BLK, width)
    q, k, v, g = (pltpu.with_memory_space_constraint(a, pltpu.HBM) for a in (q, k, v, g))
    near, far = call(
        tails_body,
        "tails",
        [((2, LEFT * SEG - SEG, width), BF16), ((2, SEG, width), BF16)],
        (k, v),
        [HBM] * 2,
        [pltpu.SemaphoreType.DMA((4,))],
        4,
    )
    ahead = [(s, s + 1) for s in range(count - 1)]
    near = lax.ppermute(near, ("z", "y"), ahead)
    far = lax.ppermute(far, ("z", "y"), ahead)
    q, k, v, g, dq2, mid, end, pay, table = call(
        own_body,
        "own",
        [((rows, width), BF16)] * 4
        + [
            ((BLK, width), BF16),
            ((2, 2 * BLK, width), F32),
            (pair, F32),
            ((2 * HEADS, BLK), F32),
            ((3 * HEADS, BLK, BLK), F32),
        ],
        (q, k, v, g, rel_bias),
        [HBM] * 4 + [VMEM],
        [pltpu.VMEM((8, 2 * BLK), F32), pltpu.SemaphoreType.DMA((4,))],
    )
    seen = (HEADS, 2 * BLK + SEG, BLK)
    dq1, part, pay, expo, dp, stat = call(
        near_body,
        "near",
        [
            ((BLK, width), BF16),
            ((2, 3 * BLK, width), F32),
            ((2 * HEADS, BLK), F32),
            (seen, F32),
            (seen, F32),
            ((8, BLK), F32),
        ],
        (q, k, v, g, near, table, mid, pay),
    )
    group = size["y"] * size["c"]
    z_order, y_order, x_order, c_order = (late_first(size[a], ORDERS[a]) for a in AXES)
    pay, prob, low, back = call(
        far_body,
        "far",
        [
            ((group, 2 * HEADS, BLK), F32),
            ((HEADS, 3 * BLK, BLK), BF16),
            ((HEADS, 3 * BLK, BLK), BF16),
            ((2, 2 * BLK, width), BF16),
        ],
        (q, g, far, table, pay, expo, dp, stat, part),
        scratch=[pltpu.VMEM((group, 2 * HEADS, BLK), F32), pltpu.SemaphoreType.DMA],
        outputs=(HBM, VMEM, VMEM, VMEM),
    )
    pay = exchange(pay, size, ("y", y_order), ("c", c_order))
    back = lax.ppermute(back, ("z", "y"), [(s + 1, s) for s in range(count - 1)])
    pay = pay.reshape(size["y"], size["c"] * 2 * HEADS, BLK).sum(axis=0)
    pay = jnp.broadcast_to(pay, (size["z"] * size["x"], *pay.shape))
    pay = exchange(pay, size, ("z", z_order), ("x", x_order))
    dq, dk, dv = call(
        join_body,
        "join",
        [((rows, width), BF16)] * 3,
        (q, k, g, near, far, part, end, prob, low, dq1, dq2, back),
    )
    (bias,) = call(
        functools.partial(table_body, x_order, c_order),
        "table",
        [((size["x"] * size["c"] * HEADS, BUCKETS), F32)],
        (pay.reshape(size["z"], size["x"] * size["c"] * 2 * HEADS, BLK),),
        scratch=[pltpu.VMEM((size["x"] * size["c"] * 2 * HEADS, BLK), F32)],
        mib=4,
    )
    return tuple(a.reshape(queries.shape) for a in (dq, dk, dv)) + (bias,)


def solution(mesh):
    sp, tp = mesh.devices.shape
    split = Mesh(mesh.devices.reshape(8, sp // 8, tp // 2, 2), AXES)
    rows = P(None, ("z", "y"), ("x", "c"))
    return jax.shard_map(
        local,
        mesh=split,
        in_specs=(rows, rows, rows, P(("x", "c"), None), rows),
        out_specs=(rows, rows, rows, P()),
        check_vma=False,
    )
```

```python
import functools
import math

import jax
import jax.numpy as jnp
from jax import lax
from jax.experimental import pallas as pl
from jax.experimental.pallas import tpu as pltpu
from jax.sharding import Mesh, PartitionSpec as P

HEAD_DIM = 128
SEG = 64
LEFT = 4
CLIP = 128
BUCKETS = 192
HEADS = 2
BLK = 128
FAR = 96
LEAD = BLK - FAR
SCALE = HEAD_DIM**-0.5
LOG2E = 1.4426950408889634
NEG = -1e30
F32 = jnp.float32
BF16 = jnp.bfloat16
VMEM = pl.BlockSpec(memory_space=pltpu.VMEM)
HBM = pl.BlockSpec(memory_space=pltpu.HBM)
AXES = ("z", "y", "x", "c")
ORDERS = {"z": (5, 3, 2, 1, 0, 4, 7, 6), "y": (4, 5, 3, 6, 2, 7, 1, 0), "x": (2, 1, 3, 0), "c": (1, 0)}


def dot(a, b, ca, cb):
    return lax.dot_general(a, b, (((ca,), (cb,)), ((), ())), preferred_element_type=F32)


def iotas():
    c = lax.broadcasted_iota(jnp.int32, (BLK, BLK), 0)
    r = lax.broadcasted_iota(jnp.int32, (BLK, BLK), 1)
    return c, r


def bias_blocks(row):
    c, r = iotas()
    row = row * LOG2E
    wide = jnp.broadcast_to(row, (8, 2 * BLK))
    mid = pltpu.roll(wide, 2 * BLK - (SEG - 1), 1)[:1, :BLK]
    low = pltpu.roll(wide, SEG + 1, 1)[:1, :BLK]
    top = wide[:1, BUCKETS - 1 : BUCKETS]
    mid = pltpu.roll(jnp.broadcast_to(mid, (BLK, BLK)), 0, 1, stride=1, stride_axis=0)
    low = pltpu.roll(jnp.broadcast_to(low, (BLK, BLK)), 0, 1, stride=1, stride_axis=0)
    t0 = jnp.where((c < SEG) & (r >= SEG), NEG, top)
    t1 = jnp.where(r >= c, top, mid)
    t2 = jnp.where(r >= c, mid, jnp.where((c >= SEG) & (r < SEG), NEG, low))
    return t0, t1, t2


def along_diagonals(x):
    acc = x[:8]
    for a in range(8, BLK, 8):
        acc = acc + pltpu.roll(x[a : a + 8], BLK - a, 1)
    row = lax.broadcasted_iota(jnp.int32, acc.shape, 0)
    out = acc
    for b in range(1, 8):
        out = jnp.where(row == b, pltpu.roll(acc, BLK - b, 1), out)
    return jnp.sum(out, axis=0, keepdims=True)


def skew_sum(d0, d1, d2):
    c, r = iotas()
    upper = r >= c
    mid = along_diagonals(jnp.where(upper, d2, d1))
    low = along_diagonals(jnp.where(upper, 0.0, d2))
    top = jnp.sum(jnp.where(upper, d1, 0.0) + d0, axis=0, keepdims=True)
    top = top + pltpu.roll(jnp.broadcast_to(top, (8, BLK)), SEG, 1)[:1]
    low = jnp.where(r[:1] < SEG, top, low)
    return jnp.concatenate([low, mid], axis=0)


def softmax_grad(expo, prob_grads, inv, delta):
    prob = [e * i for e, i in zip(expo, inv)]
    grad = [p * (g - delta) for p, g in zip(prob, prob_grads)]
    return [p.astype(BF16) for p in prob], [(g * SCALE).astype(BF16) for g in grad], grad


def peak_of(scores):
    return functools.reduce(jnp.maximum, scores).max(axis=0, keepdims=True)


def sum_of(blocks):
    return functools.reduce(jnp.add, blocks).sum(axis=0, keepdims=True)


def sum_rows(x):
    return x.sum(axis=0, keepdims=True)


def weights(scores, prob_grads):
    peak = peak_of(scores)
    expo = [jnp.exp2(s - peak) for s in scores]
    return expo, peak, sum_of(expo), sum_of([e * g for e, g in zip(expo, prob_grads)])


def cut(x):
    return [x[at : at + BLK] for at in range(0, x.shape[0], BLK)]


def stack(blocks):
    return jnp.concatenate(blocks, axis=0)


def head(h):
    return slice(h * HEAD_DIM, (h + 1) * HEAD_DIM)


def hidden_keys():
    first = (lax.axis_index("z") == 0) & (lax.axis_index("y") == 0)
    return jnp.where(first, NEG, 0.0).astype(F32)


def start_all(copies):
    for copy in copies:
        copy.start()
    return copies


def wait_all(copies):
    for copy in copies:
        copy.wait()


def tails_body(k_ref, v_ref, near_ref, far_ref, sem):
    first = k_ref.shape[0] - near_ref.shape[1] - far_ref.shape[1]
    copies = [
        pltpu.make_async_copy(ref.at[pl.ds(first + at, out.shape[1])], out.at[i], sem.at[2 * i + j])
        for i, ref in enumerate((k_ref, v_ref))
        for j, (out, at) in enumerate(((near_ref, far_ref.shape[1]), (far_ref, 0)))
    ]
    wait_all(start_all(copies))


def own_body(
    q_hbm, k_hbm, v_hbm, g_hbm, rb_ref,
    q_ref, k_ref, v_ref, g_ref, dq_ref, mid_ref, end_ref, pay_ref, tab_ref, rb_pad, sem,
):
    loads = ((k_hbm, k_ref), (q_hbm, q_ref), (v_hbm, v_ref), (g_hbm, g_ref))
    loads = start_all([pltpu.make_async_copy(x, y, sem.at[i]) for i, (x, y) in enumerate(loads)])
    rb_pad[...] = jnp.zeros_like(rb_pad)
    rb_pad[0:HEADS, 0:BUCKETS] = rb_ref[...]
    for h in range(HEADS):
        for m, block in enumerate(bias_blocks(rb_pad[h : h + 1, :])):
            tab_ref[3 * h + m] = block
    wait_all(loads)
    for h in range(HEADS):
        hs = head(h)
        table = [tab_ref[3 * h + m] for m in range(3)]
        k = k_ref[:, hs]
        q = q_ref[2 * BLK :, hs]
        g = g_ref[2 * BLK :, hs]
        scores = [s * (SCALE * LOG2E) + t for s, t in zip(cut(dot(k, q, 1, 1)), table)]
        dp = cut(dot(v_ref[:, hs], g, 1, 1))
        expo, _, total, mixed = weights(scores, dp)
        inv = 1.0 / total
        prob, low, grad = softmax_grad(expo, dp, [inv] * 3, mixed * inv)
        low = stack(low)
        dq_ref[:, hs] = dot(low, k, 0, 0).astype(BF16)
        for i, out in enumerate((dot(low, q, 1, 0), dot(stack(prob), g, 1, 0))):
            mid_ref[i, :, hs] = out[: 2 * BLK]
            end_ref[i, :, hs] = out[2 * BLK :]
        pay_ref[2 * h : 2 * h + 2, :] = skew_sum(*grad)


def near_body(
    q_ref, k_ref, v_ref, g_ref, near_ref, tab_ref, pay_in,
    prob_ref, low_ref, pay_ref, expo_ref, dp_ref, stat_ref,
):
    hidden = hidden_keys()
    for h in range(HEADS):
        hs = head(h)
        table = [tab_ref[3 * h + m] for m in range(3)]
        q = q_ref[: 2 * BLK, hs]
        g = g_ref[: 2 * BLK, hs]
        raw = dot(stack([near_ref[0, :, hs], k_ref[: 2 * BLK, hs]]), q, 1, 1)
        dps = dot(stack([near_ref[1, :, hs], v_ref[: 2 * BLK, hs]]), g, 1, 1)
        scores = [s * (SCALE * LOG2E) + t for s, t in zip(cut(raw[LEAD:, BLK:]), [table[0] + hidden] + table[1:])]
        dp = cut(dps[LEAD:, BLK:])
        expo, _, total, mixed = weights(scores, dp)
        inv = 1.0 / total
        prob, low, grad = softmax_grad(expo, dp, [inv] * 3, mixed * inv)
        prob_ref[h] = stack(prob)
        low_ref[h] = stack(low)
        pay_ref[2 * h : 2 * h + 2, :] = skew_sum(*grad) + pay_in[2 * h : 2 * h + 2, :]
        shift = stack([table[0][FAR:] + hidden, table[1] + hidden, table[2]])
        rows = shift.shape[0]
        score = raw[:rows, :BLK] * (SCALE * LOG2E) + shift
        dp = dps[:rows, :BLK]
        peak = score.max(axis=0, keepdims=True)
        expo = jnp.exp2(score - peak)
        expo_ref[h] = expo
        dp_ref[h] = dp
        for i, x in enumerate((peak, sum_rows(expo), sum_rows(expo * dp))):
            stat_ref[3 * h + i : 3 * h + i + 1, :] = x


def far_body(
    q_ref, g_ref, far_ref, tab_ref, pay_in, expo_ref, dp_ref, stat_ref, prob1_ref, low1_ref,
    pay_hbm, prob_ref, low_ref, back_ref, pay_ref, sem,
):
    hidden = hidden_keys()
    pay = []
    for h in range(HEADS):
        hs = head(h)
        score = dot(far_ref[0, :, hs], q_ref[:BLK, hs], 1, 1) * (SCALE * LOG2E) + (tab_ref[3 * h, :FAR, :] + hidden)
        dp = dot(far_ref[1, :, hs], g_ref[:BLK, hs], 1, 1)
        peak, total, mixed = (stat_ref[3 * h + i : 3 * h + i + 1, :] for i in range(3))
        top = jnp.maximum(peak, score.max(axis=0, keepdims=True))
        expo = jnp.exp2(score - top)
        fade = jnp.exp2(peak - top)
        inv = 1.0 / (total * fade + sum_rows(expo))
        delta = (mixed * fade + sum_rows(expo * dp)) * inv
        prob = stack([expo * inv, expo_ref[h] * (fade * inv)])
        grad = prob * (stack([dp, dp_ref[h]]) - delta)
        prob_ref[h] = prob.astype(BF16)
        low_ref[h] = (grad * SCALE).astype(BF16)
        pay.append(skew_sum(*cut(grad)))
    total = jnp.concatenate(pay, axis=0) + pay_in[...]
    pay_ref[...] = jnp.broadcast_to(total[None], pay_ref.shape)
    copy = pltpu.make_async_copy(pay_ref, pay_hbm, sem)
    copy.start()
    for h in range(HEADS):
        hs = head(h)
        pairs = ((low_ref, low1_ref, q_ref), (prob_ref, prob1_ref, g_ref))
        for i, (w0, w1, x) in enumerate(pairs):
            both = jnp.concatenate([w0[h, BLK : 2 * BLK, :], w1[h, :BLK, :]], axis=1)
            back_ref[i, :BLK, hs] = dot(w0[h, :BLK, :], x[:BLK, hs], 1, 0).astype(BF16)
            back_ref[i, BLK:, hs] = dot(both, x[: 2 * BLK, hs], 1, 0).astype(BF16)
    copy.wait()


def join_body(
    q_ref, k_ref, g_ref, near_ref, far_ref, mid_ref, end_ref,
    prob_ref, low_ref, prob1_ref, low1_ref, dq2_ref, back_ref,
    dq_ref, dk_ref, dv_ref,
):
    dq_ref[2 * BLK :, :] = dq2_ref[...]
    for h in range(HEADS):
        hs = head(h)
        keys = stack([far_ref[0, :, hs], near_ref[0, :, hs], k_ref[: 2 * BLK, hs]])
        dq_ref[:BLK, hs] = dot(low_ref[h], keys[: 3 * BLK], 0, 0).astype(BF16)
        dq_ref[BLK : 2 * BLK, hs] = dot(low1_ref[h], keys[BLK:], 0, 0).astype(BF16)
        pairs = ((dk_ref, low_ref, low1_ref, q_ref), (dv_ref, prob_ref, prob1_ref, g_ref))
        for i, (out, w0, w1, x) in enumerate(pairs):
            both = jnp.concatenate([w0[h, 2 * BLK :, :], w1[h, BLK : 2 * BLK, :]], axis=1)
            first = dot(both, x[: 2 * BLK, hs], 1, 0) + mid_ref[i, :BLK, hs]
            second = dot(w1[h, 2 * BLK :, :], x[BLK : 2 * BLK, hs], 1, 0) + mid_ref[i, BLK:, hs]
            out[:BLK, hs] = first.astype(BF16)
            out[BLK : 2 * BLK, hs] = (second + back_ref[i, :BLK, hs].astype(F32)).astype(BF16)
            out[2 * BLK :, hs] = (end_ref[i, :, hs] + back_ref[i, BLK:, hs].astype(F32)).astype(BF16)


def table_body(x_order, c_order, x_ref, o_ref, sum_ref):
    heads = o_ref.shape[0]
    total = jnp.sum(x_ref[...], axis=0)
    cores = len(c_order)
    span = total.shape[0] // (len(x_order) * cores)
    for i, x in enumerate(x_order):
        for j, c in enumerate(c_order):
            at, to = (i * cores + j) * span, (x * cores + c) * span
            sum_ref[to : to + span, :] = total[at : at + span]
    low = sum_ref[pl.ds(0, heads, stride=2), :]
    mid = sum_ref[pl.ds(1, heads, stride=2), :]
    lane = lax.broadcasted_iota(jnp.int32, low.shape, 1)
    top = jnp.sum(jnp.where(lane < SEG, low, 0.0), axis=1, keepdims=True)
    mid = pltpu.roll(mid, SEG - 1, 1)
    first = jnp.where(lane < SEG - 1, pltpu.roll(low, SEG - 1, 1), mid)
    last = jnp.where(lane < SEG - 1, mid, top)
    o_ref[:, :BLK] = first
    o_ref[:, BLK:] = last[:, : BUCKETS - BLK]


def call(body, name, outs, args, spaces=None, scratch=(), mib=8, outputs=None):
    return pl.pallas_call(
        body,
        out_shape=tuple(jax.ShapeDtypeStruct(*o) for o in outs),
        in_specs=spaces or [VMEM] * len(args),
        out_specs=outputs or (VMEM,) * len(outs),
        scratch_shapes=scratch,
        compiler_params=pltpu.CompilerParams(vmem_limit_bytes=mib << 20),
        name=name,
    )(*args)


def late_first(count, order):
    return [i for i in order if i < count] + [i for i in range(count) if i not in order]


def exchange(x, size, outer, inner):
    rest = [a for a in AXES if a not in (outer[0], inner[0])]
    step = {a: math.prod(size[b] for b in AXES[AXES.index(a) + 1 :]) for a in AXES}
    groups = [
        [i * step[rest[0]] + j * step[rest[1]] + m * step[outer[0]] + n * step[inner[0]] for m in outer[1] for n in inner[1]]
        for i in range(size[rest[0]])
        for j in range(size[rest[1]])
    ]
    return lax.all_to_all(x, AXES, split_axis=0, concat_axis=0, axis_index_groups=groups, tiled=True)


def local(queries, keys, values, rel_bias, out_grad):
    _, rows, width = queries.shape
    q, k, v, g = (a.reshape(rows, width) for a in (queries, keys, values, out_grad))
    size = {a: lax.axis_size(a) for a in AXES}
    count = size["z"] * size["y"]
    pair = (2, BLK, width)
    q, k, v, g = (pltpu.with_memory_space_constraint(a, pltpu.HBM) for a in (q, k, v, g))
    near, far = call(
        tails_body,
        "tails",
        [((2, LEFT * SEG - FAR, width), BF16), ((2, FAR, width), BF16)],
        (k, v),
        [HBM] * 2,
        [pltpu.SemaphoreType.DMA((4,))],
        4,
    )
    ahead = [(s, s + 1) for s in range(count - 1)]
    near = lax.ppermute(near, ("z", "y"), ahead)
    far = lax.ppermute(far, ("z", "y"), ahead)
    q, k, v, g, dq2, mid, end, pay, table = call(
        own_body,
        "own",
        [((rows, width), BF16)] * 4
        + [
            ((BLK, width), BF16),
            ((2, 2 * BLK, width), F32),
            (pair, F32),
            ((2 * HEADS, BLK), F32),
            ((3 * HEADS, BLK, BLK), F32),
        ],
        (q, k, v, g, rel_bias),
        [HBM] * 4 + [VMEM],
        [pltpu.VMEM((8, 2 * BLK), F32), pltpu.SemaphoreType.DMA((4,))],
    )
    seen = (HEADS, 2 * BLK + LEAD, BLK)
    kept = ((HEADS, 3 * BLK, BLK), BF16)
    prob1, low1, pay, expo, dp, stat = call(
        near_body,
        "near",
        [kept, kept, ((2 * HEADS, BLK), F32), (seen, F32), (seen, F32), ((8, BLK), F32)],
        (q, k, v, g, near, table, pay),
    )
    group = size["y"] * size["c"]
    z_order, y_order, x_order, c_order = (late_first(size[a], ORDERS[a]) for a in AXES)
    pay, prob, low, back = call(
        far_body,
        "far",
        [
            ((group, 2 * HEADS, BLK), F32),
            kept,
            kept,
            ((2, 2 * BLK, width), BF16),
        ],
        (q, g, far, table, pay, expo, dp, stat, prob1, low1),
        scratch=[pltpu.VMEM((group, 2 * HEADS, BLK), F32), pltpu.SemaphoreType.DMA],
        outputs=(HBM, VMEM, VMEM, VMEM),
    )
    pay = exchange(pay, size, ("y", y_order), ("c", c_order))
    back = lax.ppermute(back, ("z", "y"), [(s + 1, s) for s in range(count - 1)])
    pay = pay.reshape(size["y"], size["c"] * 2 * HEADS, BLK).sum(axis=0)
    pay = jnp.broadcast_to(pay, (size["z"] * size["x"], *pay.shape))
    pay = exchange(pay, size, ("z", z_order), ("x", x_order))
    dq, dk, dv = call(
        join_body,
        "join",
        [((rows, width), BF16)] * 3,
        (q, k, g, near, far, mid, end, prob, low, prob1, low1, dq2, back),
    )
    (bias,) = call(
        functools.partial(table_body, x_order, c_order),
        "table",
        [((size["x"] * size["c"] * HEADS, BUCKETS), F32)],
        (pay.reshape(size["z"], size["x"] * size["c"] * 2 * HEADS, BLK),),
        scratch=[pltpu.VMEM((size["x"] * size["c"] * 2 * HEADS, BLK), F32)],
        mib=4,
    )
    return tuple(a.reshape(queries.shape) for a in (dq, dk, dv)) + (bias,)


def solution(mesh):
    sp, tp = mesh.devices.shape
    split = Mesh(mesh.devices.reshape(8, sp // 8, tp // 2, 2), AXES)
    rows = P(None, ("z", "y"), ("x", "c"))
    return jax.shard_map(
        local,
        mesh=split,
        in_specs=(rows, rows, rows, P(("x", "c"), None), rows),
        out_specs=(rows, rows, rows, P()),
        check_vma=False,
    )
```

```python
import functools
import math

import jax
import jax.numpy as jnp
from jax import lax
from jax.experimental import pallas as pl
from jax.experimental.pallas import tpu as pltpu
from jax.sharding import Mesh, PartitionSpec as P

HEAD_DIM = 128
SEG = 64
LEFT = 4
CLIP = 128
BUCKETS = 192
HEADS = 2
BLK = 128
FAR = 96
LEAD = BLK - FAR
SCALE = HEAD_DIM**-0.5
LOG2E = 1.4426950408889634
NEG = -1e30
F32 = jnp.float32
BF16 = jnp.bfloat16
VMEM = pl.BlockSpec(memory_space=pltpu.VMEM)
HBM = pl.BlockSpec(memory_space=pltpu.HBM)
AXES = ("z", "y", "x", "c")
ORDERS = {"z": (5, 3, 2, 1, 0, 4, 7, 6), "y": (4, 5, 3, 6, 2, 7, 1, 0), "x": (2, 1, 3, 0), "c": (1, 0)}


def dot(a, b, ca, cb):
    return lax.dot_general(a, b, (((ca,), (cb,)), ((), ())), preferred_element_type=F32)


def iotas():
    c = lax.broadcasted_iota(jnp.int32, (BLK, BLK), 0)
    r = lax.broadcasted_iota(jnp.int32, (BLK, BLK), 1)
    return c, r


def bias_blocks(row):
    c, r = iotas()
    row = row * LOG2E
    wide = jnp.broadcast_to(row, (8, 2 * BLK))
    mid = pltpu.roll(wide, 2 * BLK - (SEG - 1), 1)[:1, :BLK]
    low = pltpu.roll(wide, SEG + 1, 1)[:1, :BLK]
    top = wide[:1, BUCKETS - 1 : BUCKETS]
    mid = pltpu.roll(jnp.broadcast_to(mid, (BLK, BLK)), 0, 1, stride=1, stride_axis=0)
    low = pltpu.roll(jnp.broadcast_to(low, (BLK, BLK)), 0, 1, stride=1, stride_axis=0)
    t0 = jnp.where((c < SEG) & (r >= SEG), NEG, top)
    t1 = jnp.where(r >= c, top, mid)
    t2 = jnp.where(r >= c, mid, jnp.where((c >= SEG) & (r < SEG), NEG, low))
    return t0, t1, t2


def along_diagonals(x):
    acc = x[:8]
    for a in range(8, BLK, 8):
        acc = acc + pltpu.roll(x[a : a + 8], BLK - a, 1)
    row = lax.broadcasted_iota(jnp.int32, acc.shape, 0)
    out = acc
    for b in range(1, 8):
        out = jnp.where(row == b, pltpu.roll(acc, BLK - b, 1), out)
    return jnp.sum(out, axis=0, keepdims=True)


def skew_sum(d0, d1, d2):
    c, r = iotas()
    upper = r >= c
    mid = along_diagonals(jnp.where(upper, d2, d1))
    low = along_diagonals(jnp.where(upper, 0.0, d2))
    top = jnp.sum(jnp.where(upper, d1, 0.0) + d0, axis=0, keepdims=True)
    top = top + pltpu.roll(jnp.broadcast_to(top, (8, BLK)), SEG, 1)[:1]
    low = jnp.where(r[:1] < SEG, top, low)
    return jnp.concatenate([low, mid], axis=0)


def softmax_grad(expo, prob_grads, inv, delta):
    prob = [e * i for e, i in zip(expo, inv)]
    grad = [p * (g - delta) for p, g in zip(prob, prob_grads)]
    return [p.astype(BF16) for p in prob], [(g * SCALE).astype(BF16) for g in grad], grad


def peak_of(scores):
    return functools.reduce(jnp.maximum, scores).max(axis=0, keepdims=True)


def sum_of(blocks):
    return functools.reduce(jnp.add, blocks).sum(axis=0, keepdims=True)


def sum_rows(x):
    return x.sum(axis=0, keepdims=True)


def weights(scores, prob_grads):
    peak = peak_of(scores)
    expo = [jnp.exp2(s - peak) for s in scores]
    return expo, peak, sum_of(expo), sum_of([e * g for e, g in zip(expo, prob_grads)])


def cut(x):
    return [x[at : at + BLK] for at in range(0, x.shape[0], BLK)]


def stack(blocks):
    return jnp.concatenate(blocks, axis=0)


def head(h):
    return slice(h * HEAD_DIM, (h + 1) * HEAD_DIM)


def hidden_keys():
    first = (lax.axis_index("z") == 0) & (lax.axis_index("y") == 0)
    return jnp.where(first, NEG, 0.0).astype(F32)


def start_all(copies):
    for copy in copies:
        copy.start()
    return copies


def wait_all(copies):
    for copy in copies:
        copy.wait()


def tails_body(k_ref, v_ref, near_ref, far_ref, sem):
    first = k_ref.shape[0] - near_ref.shape[1] - far_ref.shape[1]
    copies = []
    for out, at in ((near_ref, first + far_ref.shape[1]), (far_ref, first)):
        half = out.shape[1] // 2
        for i, ref in enumerate((k_ref, v_ref)):
            for part in (0, half):
                rows = (ref.at[pl.ds(at + part, half)], out.at[i, pl.ds(part, half)])
                copies.append(pltpu.make_async_copy(*rows, sem.at[len(copies)]))
    wait_all(start_all(copies))


def own_body(
    q_hbm, k_hbm, v_hbm, g_hbm, rb_ref,
    q_ref, k_ref, v_ref, g_ref, dq_ref, mid_ref, end_ref, pay_ref, tab_ref, rb_pad, sem,
):
    loads = ((k_hbm, k_ref), (q_hbm, q_ref), (v_hbm, v_ref), (g_hbm, g_ref))
    loads = start_all([pltpu.make_async_copy(x, y, sem.at[i]) for i, (x, y) in enumerate(loads)])
    rb_pad[...] = jnp.zeros_like(rb_pad)
    rb_pad[0:HEADS, 0:BUCKETS] = rb_ref[...]
    for h in range(HEADS):
        for m, block in enumerate(bias_blocks(rb_pad[h : h + 1, :])):
            tab_ref[3 * h + m] = block
    wait_all(loads)
    for h in range(HEADS):
        hs = head(h)
        table = [tab_ref[3 * h + m] for m in range(3)]
        k = k_ref[:, hs]
        q = q_ref[2 * BLK :, hs]
        g = g_ref[2 * BLK :, hs]
        scores = [s * (SCALE * LOG2E) + t for s, t in zip(cut(dot(k, q, 1, 1)), table)]
        dp = cut(dot(v_ref[:, hs], g, 1, 1))
        expo, _, total, mixed = weights(scores, dp)
        inv = 1.0 / total
        prob, low, grad = softmax_grad(expo, dp, [inv] * 3, mixed * inv)
        low = stack(low)
        dq_ref[:, hs] = dot(low, k, 0, 0).astype(BF16)
        for i, out in enumerate((dot(low, q, 1, 0), dot(stack(prob), g, 1, 0))):
            mid_ref[i, :, hs] = out[: 2 * BLK]
            end_ref[i, :, hs] = out[2 * BLK :]
        pay_ref[2 * h : 2 * h + 2, :] = skew_sum(*grad)


def near_body(
    q_ref, k_ref, v_ref, g_ref, near_ref, tab_ref, pay_in,
    prob_ref, low_ref, pay_ref, expo_ref, dp_ref, stat_ref,
):
    hidden = hidden_keys()
    for h in range(HEADS):
        hs = head(h)
        table = [tab_ref[3 * h + m] for m in range(3)]
        q = q_ref[: 2 * BLK, hs]
        g = g_ref[: 2 * BLK, hs]
        raw = dot(stack([near_ref[0, :, hs], k_ref[: 2 * BLK, hs]]), q, 1, 1)
        dps = dot(stack([near_ref[1, :, hs], v_ref[: 2 * BLK, hs]]), g, 1, 1)
        scores = [s * (SCALE * LOG2E) + t for s, t in zip(cut(raw[LEAD:, BLK:]), [table[0] + hidden] + table[1:])]
        dp = cut(dps[LEAD:, BLK:])
        expo, _, total, mixed = weights(scores, dp)
        inv = 1.0 / total
        prob, low, grad = softmax_grad(expo, dp, [inv] * 3, mixed * inv)
        prob_ref[h] = stack(prob)
        low_ref[h] = stack(low)
        pay_ref[2 * h : 2 * h + 2, :] = skew_sum(*grad) + pay_in[2 * h : 2 * h + 2, :]
        shift = stack([table[0][FAR:] + hidden, table[1] + hidden, table[2]])
        rows = shift.shape[0]
        score = raw[:rows, :BLK] * (SCALE * LOG2E) + shift
        dp = dps[:rows, :BLK]
        peak = score.max(axis=0, keepdims=True)
        expo = jnp.exp2(score - peak)
        expo_ref[h] = expo
        dp_ref[h] = dp
        for i, x in enumerate((peak, sum_rows(expo), sum_rows(expo * dp))):
            stat_ref[3 * h + i : 3 * h + i + 1, :] = x


def far_body(
    q_ref, g_ref, far_ref, tab_ref, pay_in, expo_ref, dp_ref, stat_ref, prob1_ref, low1_ref,
    pay_hbm, prob_ref, low_ref, back_ref, pay_ref, sem,
):
    hidden = hidden_keys()
    pay = []
    for h in range(HEADS):
        hs = head(h)
        score = dot(far_ref[0, :, hs], q_ref[:BLK, hs], 1, 1) * (SCALE * LOG2E) + (tab_ref[3 * h, :FAR, :] + hidden)
        dp = dot(far_ref[1, :, hs], g_ref[:BLK, hs], 1, 1)
        peak, total, mixed = (stat_ref[3 * h + i : 3 * h + i + 1, :] for i in range(3))
        top = jnp.maximum(peak, score.max(axis=0, keepdims=True))
        expo = jnp.exp2(score - top)
        fade = jnp.exp2(peak - top)
        inv = 1.0 / (total * fade + sum_rows(expo))
        delta = (mixed * fade + sum_rows(expo * dp)) * inv
        prob = stack([expo * inv, expo_ref[h] * (fade * inv)])
        grad = prob * (stack([dp, dp_ref[h]]) - delta)
        prob_ref[h] = prob.astype(BF16)
        low_ref[h] = (grad * SCALE).astype(BF16)
        pay.append(skew_sum(*cut(grad)))
    total = jnp.concatenate(pay, axis=0) + pay_in[...]
    pay_ref[...] = jnp.broadcast_to(total[None], pay_ref.shape)
    copy = pltpu.make_async_copy(pay_ref, pay_hbm, sem)
    copy.start()

    def halo(h, carry):
        hs = pl.ds(pl.multiple_of(h * HEAD_DIM, HEAD_DIM), HEAD_DIM)
        pairs = ((low_ref, low1_ref, q_ref), (prob_ref, prob1_ref, g_ref))
        for i, (w0, w1, x) in enumerate(pairs):
            both = jnp.concatenate([w0[h, BLK : 2 * BLK, :], w1[h, :BLK, :]], axis=1)
            back_ref[i, :BLK, hs] = dot(w0[h, :BLK, :], x[:BLK, hs], 1, 0).astype(BF16)
            back_ref[i, BLK:, hs] = dot(both, x[: 2 * BLK, hs], 1, 0).astype(BF16)
        return carry

    lax.fori_loop(0, HEADS, halo, 0)
    copy.wait()


def join_body(
    q_ref, k_ref, g_ref, near_ref, far_ref, mid_ref, end_ref,
    prob_ref, low_ref, prob1_ref, low1_ref, dq2_ref, back_ref,
    dq_ref, dk_ref, dv_ref,
):
    dq_ref[2 * BLK :, :] = dq2_ref[...]
    for h in range(HEADS):
        hs = head(h)
        keys = stack([far_ref[0, :, hs], near_ref[0, :, hs], k_ref[: 2 * BLK, hs]])
        dq_ref[:BLK, hs] = dot(low_ref[h], keys[: 3 * BLK], 0, 0).astype(BF16)
        dq_ref[BLK : 2 * BLK, hs] = dot(low1_ref[h], keys[BLK:], 0, 0).astype(BF16)
        pairs = ((dk_ref, low_ref, low1_ref, q_ref), (dv_ref, prob_ref, prob1_ref, g_ref))
        for i, (out, w0, w1, x) in enumerate(pairs):
            both = jnp.concatenate([w0[h, 2 * BLK :, :], w1[h, BLK : 2 * BLK, :]], axis=1)
            first = dot(both, x[: 2 * BLK, hs], 1, 0) + mid_ref[i, :BLK, hs]
            second = dot(w1[h, 2 * BLK :, :], x[BLK : 2 * BLK, hs], 1, 0) + mid_ref[i, BLK:, hs]
            out[:BLK, hs] = first.astype(BF16)
            out[BLK : 2 * BLK, hs] = (second + back_ref[i, :BLK, hs].astype(F32)).astype(BF16)
            out[2 * BLK :, hs] = (end_ref[i, :, hs] + back_ref[i, BLK:, hs].astype(F32)).astype(BF16)


def table_body(x_order, c_order, x_ref, o_ref, sum_ref):
    heads = o_ref.shape[0]
    total = jnp.sum(x_ref[...], axis=0)
    cores = len(c_order)
    span = total.shape[0] // (len(x_order) * cores)
    for i, x in enumerate(x_order):
        for j, c in enumerate(c_order):
            at, to = (i * cores + j) * span, (x * cores + c) * span
            sum_ref[to : to + span, :] = total[at : at + span]
    low = sum_ref[pl.ds(0, heads, stride=2), :]
    mid = sum_ref[pl.ds(1, heads, stride=2), :]
    lane = lax.broadcasted_iota(jnp.int32, low.shape, 1)
    top = jnp.sum(jnp.where(lane < SEG, low, 0.0), axis=1, keepdims=True)
    mid = pltpu.roll(mid, SEG - 1, 1)
    first = jnp.where(lane < SEG - 1, pltpu.roll(low, SEG - 1, 1), mid)
    last = jnp.where(lane < SEG - 1, mid, top)
    o_ref[:, :BLK] = first
    o_ref[:, BLK:] = last[:, : BUCKETS - BLK]


def call(body, name, outs, args, spaces=None, scratch=(), mib=8, outputs=None):
    return pl.pallas_call(
        body,
        out_shape=tuple(jax.ShapeDtypeStruct(*o) for o in outs),
        in_specs=spaces or [VMEM] * len(args),
        out_specs=outputs or (VMEM,) * len(outs),
        scratch_shapes=scratch,
        compiler_params=pltpu.CompilerParams(vmem_limit_bytes=mib << 20),
        name=name,
    )(*args)


def late_first(count, order):
    return [i for i in order if i < count] + [i for i in range(count) if i not in order]


def exchange(x, size, outer, inner):
    rest = [a for a in AXES if a not in (outer[0], inner[0])]
    step = {a: math.prod(size[b] for b in AXES[AXES.index(a) + 1 :]) for a in AXES}
    groups = [
        [i * step[rest[0]] + j * step[rest[1]] + m * step[outer[0]] + n * step[inner[0]] for m in outer[1] for n in inner[1]]
        for i in range(size[rest[0]])
        for j in range(size[rest[1]])
    ]
    return lax.all_to_all(x, AXES, split_axis=0, concat_axis=0, axis_index_groups=groups, tiled=True)


def local(queries, keys, values, rel_bias, out_grad):
    _, rows, width = queries.shape
    q, k, v, g = (a.reshape(rows, width) for a in (queries, keys, values, out_grad))
    size = {a: lax.axis_size(a) for a in AXES}
    count = size["z"] * size["y"]
    pair = (2, BLK, width)
    q, k, v, g = (pltpu.with_memory_space_constraint(a, pltpu.HBM) for a in (q, k, v, g))
    near, far = call(
        tails_body,
        "tails",
        [((2, LEFT * SEG - FAR, width), BF16), ((2, FAR, width), BF16)],
        (k, v),
        [HBM] * 2,
        [pltpu.SemaphoreType.DMA((8,))],
        4,
    )
    ahead = [(s, s + 1) for s in range(count - 1)]
    near = lax.ppermute(near, ("z", "y"), ahead)
    far = lax.ppermute(far, ("z", "y"), ahead)
    q, k, v, g, dq2, mid, end, pay, table = call(
        own_body,
        "own",
        [((rows, width), BF16)] * 4
        + [
            ((BLK, width), BF16),
            ((2, 2 * BLK, width), F32),
            (pair, F32),
            ((2 * HEADS, BLK), F32),
            ((3 * HEADS, BLK, BLK), F32),
        ],
        (q, k, v, g, rel_bias),
        [HBM] * 4 + [VMEM],
        [pltpu.VMEM((8, 2 * BLK), F32), pltpu.SemaphoreType.DMA((4,))],
    )
    seen = (HEADS, 2 * BLK + LEAD, BLK)
    kept = ((HEADS, 3 * BLK, BLK), BF16)
    prob1, low1, pay, expo, dp, stat = call(
        near_body,
        "near",
        [kept, kept, ((2 * HEADS, BLK), F32), (seen, F32), (seen, F32), ((8, BLK), F32)],
        (q, k, v, g, near, table, pay),
    )
    group = size["y"] * size["c"]
    z_order, y_order, x_order, c_order = (late_first(size[a], ORDERS[a]) for a in AXES)
    pay, prob, low, back = call(
        far_body,
        "far",
        [
            ((group, 2 * HEADS, BLK), F32),
            kept,
            kept,
            ((2, 2 * BLK, width), BF16),
        ],
        (q, g, far, table, pay, expo, dp, stat, prob1, low1),
        scratch=[pltpu.VMEM((group, 2 * HEADS, BLK), F32), pltpu.SemaphoreType.DMA],
        outputs=(HBM, VMEM, VMEM, VMEM),
    )
    pay = exchange(pay, size, ("y", y_order), ("c", c_order))
    back = lax.ppermute(back, ("z", "y"), [(s + 1, s) for s in range(count - 1)])
    pay = pay.reshape(size["y"], size["c"] * 2 * HEADS, BLK).sum(axis=0)
    pay = jnp.broadcast_to(pay, (size["z"] * size["x"], *pay.shape))
    pay = exchange(pay, size, ("z", z_order), ("x", x_order))
    dq, dk, dv = call(
        join_body,
        "join",
        [((rows, width), BF16)] * 3,
        (q, k, g, near, far, mid, end, prob, low, prob1, low1, dq2, back),
    )
    (bias,) = call(
        functools.partial(table_body, x_order, c_order),
        "table",
        [((size["x"] * size["c"] * HEADS, BUCKETS), F32)],
        (pay.reshape(size["z"], size["x"] * size["c"] * 2 * HEADS, BLK),),
        scratch=[pltpu.VMEM((size["x"] * size["c"] * 2 * HEADS, BLK), F32)],
        mib=4,
    )
    return tuple(a.reshape(queries.shape) for a in (dq, dk, dv)) + (bias,)


def solution(mesh):
    sp, tp = mesh.devices.shape
    split = Mesh(mesh.devices.reshape(8, sp // 8, tp // 2, 2), AXES)
    rows = P(None, ("z", "y"), ("x", "c"))
    return jax.shard_map(
        local,
        mesh=split,
        in_specs=(rows, rows, rows, P(("x", "c"), None), rows),
        out_specs=(rows, rows, rows, P()),
        check_vma=False,
    )
```

```python
import functools
import math

import jax
import jax.numpy as jnp
from jax import lax
from jax.experimental import pallas as pl
from jax.experimental.pallas import tpu as pltpu
from jax.sharding import Mesh, PartitionSpec as P

HEAD_DIM = 128
SEG = 64
LEFT = 4
CLIP = 128
BUCKETS = 192
HEADS = 2
BLK = 128
FAR = 96
LEAD = BLK - FAR
SCALE = HEAD_DIM**-0.5
LOG2E = 1.4426950408889634
NEG = -1e30
F32 = jnp.float32
BF16 = jnp.bfloat16
VMEM = pl.BlockSpec(memory_space=pltpu.VMEM)
HBM = pl.BlockSpec(memory_space=pltpu.HBM)
AXES = ("z", "y", "x", "c")
ORDERS = {"z": (5, 3, 2, 1, 0, 4, 7, 6), "y": (4, 5, 3, 6, 2, 7, 1, 0), "x": (2, 1, 3, 0), "c": (1, 0)}


def dot(a, b, ca, cb):
    return lax.dot_general(a, b, (((ca,), (cb,)), ((), ())), preferred_element_type=F32)


def iotas():
    c = lax.broadcasted_iota(jnp.int32, (BLK, BLK), 0)
    r = lax.broadcasted_iota(jnp.int32, (BLK, BLK), 1)
    return c, r


def bias_blocks(row):
    c, r = iotas()
    row = row * LOG2E
    wide = jnp.broadcast_to(row, (8, 2 * BLK))
    mid = pltpu.roll(wide, 2 * BLK - (SEG - 1), 1)[:1, :BLK]
    low = pltpu.roll(wide, SEG + 1, 1)[:1, :BLK]
    top = wide[:1, BUCKETS - 1 : BUCKETS]
    mid = pltpu.roll(jnp.broadcast_to(mid, (BLK, BLK)), 0, 1, stride=1, stride_axis=0)
    low = pltpu.roll(jnp.broadcast_to(low, (BLK, BLK)), 0, 1, stride=1, stride_axis=0)
    t0 = jnp.where((c < SEG) & (r >= SEG), NEG, top)
    t1 = jnp.where(r >= c, top, mid)
    t2 = jnp.where(r >= c, mid, jnp.where((c >= SEG) & (r < SEG), NEG, low))
    return t0, t1, t2


def tree_sum(parts):
    while len(parts) > 1:
        parts = [sum(parts[i : i + 2][1:], parts[i]) for i in range(0, len(parts), 2)]
    return parts[0]


def along_diagonals(x):
    acc = tree_sum([pltpu.roll(x[a : a + 8], BLK - a, 1) if a else x[:8] for a in range(0, BLK, 8)])
    row = lax.broadcasted_iota(jnp.int32, acc.shape, 0)
    parts = [jnp.where(row == b, pltpu.roll(acc, BLK - b, 1) if b else acc, 0.0) for b in range(8)]
    return jnp.sum(tree_sum(parts), axis=0, keepdims=True)


def skew_sum(d0, d1, d2):
    c, r = iotas()
    upper = r >= c
    mid = along_diagonals(jnp.where(upper, d2, d1))
    low = along_diagonals(jnp.where(upper, 0.0, d2))
    top = jnp.sum(jnp.where(upper, d1, 0.0) + d0, axis=0, keepdims=True)
    top = top + pltpu.roll(jnp.broadcast_to(top, (8, BLK)), SEG, 1)[:1]
    low = jnp.where(r[:1] < SEG, top, low)
    return jnp.concatenate([low, mid], axis=0)


def softmax_grad(expo, prob_grads, inv, delta):
    prob = [e * i for e, i in zip(expo, inv)]
    grad = [p * (g - delta) for p, g in zip(prob, prob_grads)]
    return [p.astype(BF16) for p in prob], [(g * SCALE).astype(BF16) for g in grad], grad


def peak_of(scores):
    return functools.reduce(jnp.maximum, scores).max(axis=0, keepdims=True)


def sum_of(blocks):
    return functools.reduce(jnp.add, blocks).sum(axis=0, keepdims=True)


def sum_rows(x):
    return x.sum(axis=0, keepdims=True)


def weights(scores, prob_grads):
    peak = peak_of(scores)
    expo = [jnp.exp2(s - peak) for s in scores]
    return expo, peak, sum_of(expo), sum_of([e * g for e, g in zip(expo, prob_grads)])


def cut(x):
    return [x[at : at + BLK] for at in range(0, x.shape[0], BLK)]


def stack(blocks):
    return jnp.concatenate(blocks, axis=0)


def head(h):
    return slice(h * HEAD_DIM, (h + 1) * HEAD_DIM)


def hidden_keys():
    first = (lax.axis_index("z") == 0) & (lax.axis_index("y") == 0)
    return jnp.where(first, NEG, 0.0).astype(F32)


def start_all(copies):
    for copy in copies:
        copy.start()
    return copies


def wait_all(copies):
    for copy in copies:
        copy.wait()


def tails_body(k_ref, v_ref, near_ref, far_ref, sem):
    first = k_ref.shape[0] - near_ref.shape[1] - far_ref.shape[1]
    copies = []
    for out, at in ((near_ref, first + far_ref.shape[1]), (far_ref, first)):
        half = out.shape[1] // 2
        for i, ref in enumerate((k_ref, v_ref)):
            for part in (0, half):
                rows = (ref.at[pl.ds(at + part, half)], out.at[i, pl.ds(part, half)])
                copies.append(pltpu.make_async_copy(*rows, sem.at[len(copies)]))
    wait_all(start_all(copies))


def own_body(
    q_hbm, k_hbm, v_hbm, g_hbm, rb_ref,
    q_ref, k_ref, v_ref, g_ref, dq_ref, mid_ref, end_ref, pay_ref, tab_ref, rb_pad, sem,
):
    loads = ((k_hbm, k_ref), (q_hbm, q_ref), (v_hbm, v_ref), (g_hbm, g_ref))
    loads = start_all([pltpu.make_async_copy(x, y, sem.at[i]) for i, (x, y) in enumerate(loads)])
    rb_pad[...] = jnp.zeros_like(rb_pad)
    rb_pad[0:HEADS, 0:BUCKETS] = rb_ref[...]
    for h in range(HEADS):
        for m, block in enumerate(bias_blocks(rb_pad[h : h + 1, :])):
            tab_ref[3 * h + m] = block
    wait_all(loads)
    for h in range(HEADS):
        hs = head(h)
        table = [tab_ref[3 * h + m] for m in range(3)]
        k = k_ref[:, hs]
        q = q_ref[2 * BLK :, hs]
        g = g_ref[2 * BLK :, hs]
        scores = [s * (SCALE * LOG2E) + t for s, t in zip(cut(dot(k, q, 1, 1)), table)]
        dp = cut(dot(v_ref[:, hs], g, 1, 1))
        expo, _, total, mixed = weights(scores, dp)
        inv = 1.0 / total
        prob, low, grad = softmax_grad(expo, dp, [inv] * 3, mixed * inv)
        low = stack(low)
        dq_ref[:, hs] = dot(low, k, 0, 0).astype(BF16)
        for i, out in enumerate((dot(low, q, 1, 0), dot(stack(prob), g, 1, 0))):
            mid_ref[i, :, hs] = out[: 2 * BLK]
            end_ref[i, :, hs] = out[2 * BLK :]
        pay_ref[2 * h : 2 * h + 2, :] = skew_sum(*grad)


def near_body(
    q_ref, k_ref, v_ref, g_ref, near_ref, tab_ref, pay_in,
    prob_ref, low_ref, pay_ref, expo_ref, dp_ref, stat_ref,
):
    hidden = hidden_keys()
    for h in range(HEADS):
        hs = head(h)
        table = [tab_ref[3 * h + m] for m in range(3)]
        q = q_ref[: 2 * BLK, hs]
        g = g_ref[: 2 * BLK, hs]
        raw = dot(stack([near_ref[0, :, hs], k_ref[: 2 * BLK, hs]]), q, 1, 1)
        dps = dot(stack([near_ref[1, :, hs], v_ref[: 2 * BLK, hs]]), g, 1, 1)
        scores = [s * (SCALE * LOG2E) + t for s, t in zip(cut(raw[LEAD:, BLK:]), [table[0] + hidden] + table[1:])]
        dp = cut(dps[LEAD:, BLK:])
        expo, _, total, mixed = weights(scores, dp)
        inv = 1.0 / total
        prob, low, grad = softmax_grad(expo, dp, [inv] * 3, mixed * inv)
        prob_ref[h] = stack(prob)
        low_ref[h] = stack(low)
        pay_ref[2 * h : 2 * h + 2, :] = skew_sum(*grad) + pay_in[2 * h : 2 * h + 2, :]
        shift = stack([table[0][FAR:] + hidden, table[1] + hidden, table[2]])
        rows = shift.shape[0]
        score = raw[:rows, :BLK] * (SCALE * LOG2E) + shift
        dp = dps[:rows, :BLK]
        peak = score.max(axis=0, keepdims=True)
        expo = jnp.exp2(score - peak)
        expo_ref[h] = expo
        dp_ref[h] = dp
        for i, x in enumerate((peak, sum_rows(expo), sum_rows(expo * dp))):
            stat_ref[3 * h + i : 3 * h + i + 1, :] = x


def far_body(
    q_ref, g_ref, far_ref, tab_ref, pay_in, expo_ref, dp_ref, stat_ref, prob1_ref, low1_ref,
    pay_hbm, prob_ref, low_ref, back_ref, pay_ref, sem,
):
    hidden = hidden_keys()
    pay = []
    for h in range(HEADS):
        hs = head(h)
        score = dot(far_ref[0, :, hs], q_ref[:BLK, hs], 1, 1) * (SCALE * LOG2E) + (tab_ref[3 * h, :FAR, :] + hidden)
        dp = dot(far_ref[1, :, hs], g_ref[:BLK, hs], 1, 1)
        peak, total, mixed = (stat_ref[3 * h + i : 3 * h + i + 1, :] for i in range(3))
        top = jnp.maximum(peak, score.max(axis=0, keepdims=True))
        expo = jnp.exp2(score - top)
        fade = jnp.exp2(peak - top)
        inv = 1.0 / (total * fade + sum_rows(expo))
        delta = (mixed * fade + sum_rows(expo * dp)) * inv
        prob = stack([expo * inv, expo_ref[h] * (fade * inv)])
        grad = prob * (stack([dp, dp_ref[h]]) - delta)
        prob_ref[h] = prob.astype(BF16)
        low_ref[h] = (grad * SCALE).astype(BF16)
        pay.append(skew_sum(*cut(grad)))
    total = jnp.concatenate(pay, axis=0) + pay_in[...]
    pay_ref[...] = jnp.broadcast_to(total[None], pay_ref.shape)
    copy = pltpu.make_async_copy(pay_ref, pay_hbm, sem)
    copy.start()

    def halo(h, carry):
        hs = pl.ds(pl.multiple_of(h * HEAD_DIM, HEAD_DIM), HEAD_DIM)
        pairs = ((low_ref, low1_ref, q_ref), (prob_ref, prob1_ref, g_ref))
        for i, (w0, w1, x) in enumerate(pairs):
            both = jnp.concatenate([w0[h, BLK : 2 * BLK, :], w1[h, :BLK, :]], axis=1)
            back_ref[i, :BLK, hs] = dot(w0[h, :BLK, :], x[:BLK, hs], 1, 0).astype(BF16)
            back_ref[i, BLK:, hs] = dot(both, x[: 2 * BLK, hs], 1, 0).astype(BF16)
        return carry

    lax.fori_loop(0, HEADS, halo, 0)
    copy.wait()


def join_body(
    q_ref, k_ref, g_ref, near_ref, far_ref, mid_ref, end_ref,
    prob_ref, low_ref, prob1_ref, low1_ref, dq2_ref, back_ref,
    dq_ref, dk_ref, dv_ref,
):
    dq_ref[2 * BLK :, :] = dq2_ref[...]
    for h in range(HEADS):
        hs = head(h)
        keys = stack([far_ref[0, :, hs], near_ref[0, :, hs], k_ref[: 2 * BLK, hs]])
        dq_ref[:BLK, hs] = dot(low_ref[h], keys[: 3 * BLK], 0, 0).astype(BF16)
        dq_ref[BLK : 2 * BLK, hs] = dot(low1_ref[h], keys[BLK:], 0, 0).astype(BF16)
        pairs = ((dk_ref, low_ref, low1_ref, q_ref), (dv_ref, prob_ref, prob1_ref, g_ref))
        for i, (out, w0, w1, x) in enumerate(pairs):
            both = jnp.concatenate([w0[h, 2 * BLK :, :], w1[h, BLK : 2 * BLK, :]], axis=1)
            first = dot(both, x[: 2 * BLK, hs], 1, 0) + mid_ref[i, :BLK, hs]
            second = dot(w1[h, 2 * BLK :, :], x[BLK : 2 * BLK, hs], 1, 0) + mid_ref[i, BLK:, hs]
            out[:BLK, hs] = first.astype(BF16)
            out[BLK : 2 * BLK, hs] = (second + back_ref[i, :BLK, hs].astype(F32)).astype(BF16)
            out[2 * BLK :, hs] = (end_ref[i, :, hs] + back_ref[i, BLK:, hs].astype(F32)).astype(BF16)


def table_body(x_order, c_order, x_ref, o_ref, sum_ref):
    heads = o_ref.shape[0]
    total = jnp.sum(x_ref[...], axis=0)
    cores = len(c_order)
    span = total.shape[0] // (len(x_order) * cores)
    for i, x in enumerate(x_order):
        for j, c in enumerate(c_order):
            at, to = (i * cores + j) * span, (x * cores + c) * span
            sum_ref[to : to + span, :] = total[at : at + span]
    low = sum_ref[pl.ds(0, heads, stride=2), :]
    mid = sum_ref[pl.ds(1, heads, stride=2), :]
    lane = lax.broadcasted_iota(jnp.int32, low.shape, 1)
    top = jnp.sum(jnp.where(lane < SEG, low, 0.0), axis=1, keepdims=True)
    mid = pltpu.roll(mid, SEG - 1, 1)
    first = jnp.where(lane < SEG - 1, pltpu.roll(low, SEG - 1, 1), mid)
    last = jnp.where(lane < SEG - 1, mid, top)
    o_ref[:, :BLK] = first
    o_ref[:, BLK:] = last[:, : BUCKETS - BLK]


def call(body, name, outs, args, spaces=None, scratch=(), mib=8, outputs=None):
    return pl.pallas_call(
        body,
        out_shape=tuple(jax.ShapeDtypeStruct(*o) for o in outs),
        in_specs=spaces or [VMEM] * len(args),
        out_specs=outputs or (VMEM,) * len(outs),
        scratch_shapes=scratch,
        compiler_params=pltpu.CompilerParams(vmem_limit_bytes=mib << 20),
        name=name,
    )(*args)


def late_first(count, order):
    return [i for i in order if i < count] + [i for i in range(count) if i not in order]


def exchange(x, size, outer, inner):
    rest = [a for a in AXES if a not in (outer[0], inner[0])]
    step = {a: math.prod(size[b] for b in AXES[AXES.index(a) + 1 :]) for a in AXES}
    groups = [
        [i * step[rest[0]] + j * step[rest[1]] + m * step[outer[0]] + n * step[inner[0]] for m in outer[1] for n in inner[1]]
        for i in range(size[rest[0]])
        for j in range(size[rest[1]])
    ]
    return lax.all_to_all(x, AXES, split_axis=0, concat_axis=0, axis_index_groups=groups, tiled=True)


def local(queries, keys, values, rel_bias, out_grad):
    _, rows, width = queries.shape
    q, k, v, g = (a.reshape(rows, width) for a in (queries, keys, values, out_grad))
    size = {a: lax.axis_size(a) for a in AXES}
    count = size["z"] * size["y"]
    pair = (2, BLK, width)
    q, k, v, g = (pltpu.with_memory_space_constraint(a, pltpu.HBM) for a in (q, k, v, g))
    near, far = call(
        tails_body,
        "tails",
        [((2, LEFT * SEG - FAR, width), BF16), ((2, FAR, width), BF16)],
        (k, v),
        [HBM] * 2,
        [pltpu.SemaphoreType.DMA((8,))],
        4,
    )
    ahead = [(s, s + 1) for s in range(count - 1)]
    near = lax.ppermute(near, ("z", "y"), ahead)
    far = lax.ppermute(far, ("z", "y"), ahead)
    q, k, v, g, dq2, mid, end, pay, table = call(
        own_body,
        "own",
        [((rows, width), BF16)] * 4
        + [
            ((BLK, width), BF16),
            ((2, 2 * BLK, width), F32),
            (pair, F32),
            ((2 * HEADS, BLK), F32),
            ((3 * HEADS, BLK, BLK), F32),
        ],
        (q, k, v, g, rel_bias),
        [HBM] * 4 + [VMEM],
        [pltpu.VMEM((8, 2 * BLK), F32), pltpu.SemaphoreType.DMA((4,))],
    )
    seen = (HEADS, 2 * BLK + LEAD, BLK)
    kept = ((HEADS, 3 * BLK, BLK), BF16)
    prob1, low1, pay, expo, dp, stat = call(
        near_body,
        "near",
        [kept, kept, ((2 * HEADS, BLK), F32), (seen, F32), (seen, F32), ((8, BLK), F32)],
        (q, k, v, g, near, table, pay),
    )
    group = size["y"] * size["c"]
    z_order, y_order, x_order, c_order = (late_first(size[a], ORDERS[a]) for a in AXES)
    pay, prob, low, back = call(
        far_body,
        "far",
        [
            ((group, 2 * HEADS, BLK), F32),
            kept,
            kept,
            ((2, 2 * BLK, width), BF16),
        ],
        (q, g, far, table, pay, expo, dp, stat, prob1, low1),
        scratch=[pltpu.VMEM((group, 2 * HEADS, BLK), F32), pltpu.SemaphoreType.DMA],
        outputs=(HBM, VMEM, VMEM, VMEM),
    )
    pay = exchange(pay, size, ("y", y_order), ("c", c_order))
    back = lax.ppermute(back, ("z", "y"), [(s + 1, s) for s in range(count - 1)])
    pay = pay.reshape(size["y"], size["c"] * 2 * HEADS, BLK).sum(axis=0)
    pay = jnp.broadcast_to(pay, (size["z"] * size["x"], *pay.shape))
    pay = exchange(pay, size, ("z", z_order), ("x", x_order))
    dq, dk, dv = call(
        join_body,
        "join",
        [((rows, width), BF16)] * 3,
        (q, k, g, near, far, mid, end, prob, low, prob1, low1, dq2, back),
    )
    (bias,) = call(
        functools.partial(table_body, x_order, c_order),
        "table",
        [((size["x"] * size["c"] * HEADS, BUCKETS), F32)],
        (pay.reshape(size["z"], size["x"] * size["c"] * 2 * HEADS, BLK),),
        scratch=[pltpu.VMEM((size["x"] * size["c"] * 2 * HEADS, BLK), F32)],
        mib=4,
    )
    return tuple(a.reshape(queries.shape) for a in (dq, dk, dv)) + (bias,)


def solution(mesh):
    sp, tp = mesh.devices.shape
    split = Mesh(mesh.devices.reshape(8, sp // 8, tp // 2, 2), AXES)
    rows = P(None, ("z", "y"), ("x", "c"))
    return jax.shard_map(
        local,
        mesh=split,
        in_specs=(rows, rows, rows, P(("x", "c"), None), rows),
        out_specs=(rows, rows, rows, P()),
        check_vma=False,
    )
```

```python
import functools
import math

import jax
import jax.numpy as jnp
from jax import lax
from jax.experimental import pallas as pl
from jax.experimental.pallas import tpu as pltpu
from jax.sharding import Mesh, PartitionSpec as P

HEAD_DIM = 128
SEG = 64
LEFT = 4
CLIP = 128
BUCKETS = 192
HEADS = 2
BLK = 128
FAR = 112
LEAD = BLK - FAR
SCALE = HEAD_DIM**-0.5
LOG2E = 1.4426950408889634
NEG = -1e30
F32 = jnp.float32
BF16 = jnp.bfloat16
VMEM = pl.BlockSpec(memory_space=pltpu.VMEM)
HBM = pl.BlockSpec(memory_space=pltpu.HBM)
AXES = ("z", "y", "x", "c")
ORDERS = {"z": (5, 3, 2, 1, 0, 4, 7, 6), "y": (4, 5, 3, 6, 2, 7, 1, 0), "x": (2, 1, 3, 0), "c": (1, 0)}


def dot(a, b, ca, cb):
    return lax.dot_general(a, b, (((ca,), (cb,)), ((), ())), preferred_element_type=F32)


def iotas():
    c = lax.broadcasted_iota(jnp.int32, (BLK, BLK), 0)
    r = lax.broadcasted_iota(jnp.int32, (BLK, BLK), 1)
    return c, r


def bias_blocks(row):
    c, r = iotas()
    row = row * LOG2E
    wide = jnp.broadcast_to(row, (8, 2 * BLK))
    mid = pltpu.roll(wide, 2 * BLK - (SEG - 1), 1)[:1, :BLK]
    low = pltpu.roll(wide, SEG + 1, 1)[:1, :BLK]
    top = wide[:1, BUCKETS - 1 : BUCKETS]
    mid = pltpu.roll(jnp.broadcast_to(mid, (BLK, BLK)), 0, 1, stride=1, stride_axis=0)
    low = pltpu.roll(jnp.broadcast_to(low, (BLK, BLK)), 0, 1, stride=1, stride_axis=0)
    t0 = jnp.where((c < SEG) & (r >= SEG), NEG, top)
    t1 = jnp.where(r >= c, top, mid)
    t2 = jnp.where(r >= c, mid, jnp.where((c >= SEG) & (r < SEG), NEG, low))
    return t0, t1, t2


def along_diagonals(x):
    acc = x[:8]
    for a in range(8, BLK, 8):
        acc = acc + pltpu.roll(x[a : a + 8], BLK - a, 1)
    row = lax.broadcasted_iota(jnp.int32, acc.shape, 0)
    out = acc
    for b in range(1, 8):
        out = jnp.where(row == b, pltpu.roll(acc, BLK - b, 1), out)
    return jnp.sum(out, axis=0, keepdims=True)


def skew_sum(d0, d1, d2):
    c, r = iotas()
    upper = r >= c
    mid = along_diagonals(jnp.where(upper, d2, d1))
    low = along_diagonals(jnp.where(upper, 0.0, d2))
    top = jnp.sum(jnp.where(upper, d1, 0.0) + d0, axis=0, keepdims=True)
    top = top + pltpu.roll(jnp.broadcast_to(top, (8, BLK)), SEG, 1)[:1]
    low = jnp.where(r[:1] < SEG, top, low)
    return jnp.concatenate([low, mid], axis=0)


def softmax_grad(expo, prob_grads, inv, delta):
    prob = [e * i for e, i in zip(expo, inv)]
    grad = [p * (g - delta) for p, g in zip(prob, prob_grads)]
    return [p.astype(BF16) for p in prob], [(g * SCALE).astype(BF16) for g in grad], grad


def peak_of(scores):
    return functools.reduce(jnp.maximum, scores).max(axis=0, keepdims=True)


def sum_of(blocks):
    return functools.reduce(jnp.add, blocks).sum(axis=0, keepdims=True)


def sum_rows(x):
    return x.sum(axis=0, keepdims=True)


def weights(scores, prob_grads):
    peak = peak_of(scores)
    expo = [jnp.exp2(s - peak) for s in scores]
    return expo, peak, sum_of(expo), sum_of([e * g for e, g in zip(expo, prob_grads)])


def cut(x):
    return [x[at : at + BLK] for at in range(0, x.shape[0], BLK)]


def stack(blocks):
    return jnp.concatenate(blocks, axis=0)


def head(h):
    return slice(h * HEAD_DIM, (h + 1) * HEAD_DIM)


def hidden_keys():
    first = (lax.axis_index("z") == 0) & (lax.axis_index("y") == 0)
    return jnp.where(first, NEG, 0.0).astype(F32)


def start_all(copies):
    for copy in copies:
        copy.start()
    return copies


def wait_all(copies):
    for copy in copies:
        copy.wait()


def tails_body(k_ref, v_ref, near_ref, far_ref, sem):
    first = k_ref.shape[0] - near_ref.shape[1] - far_ref.shape[1]
    copies = []
    for out, at in ((near_ref, first + far_ref.shape[1]), (far_ref, first)):
        half = out.shape[1] // 2
        for i, ref in enumerate((k_ref, v_ref)):
            for part in (0, half):
                rows = (ref.at[pl.ds(at + part, half)], out.at[i, pl.ds(part, half)])
                copies.append(pltpu.make_async_copy(*rows, sem.at[len(copies)]))
    wait_all(start_all(copies))


def own_body(
    q_hbm, k_hbm, v_hbm, g_hbm, rb_ref,
    q_ref, k_ref, v_ref, g_ref, dq_ref, mid_ref, end_ref, pay_ref, tab_ref, rb_pad, sem,
):
    loads = ((k_hbm, k_ref), (q_hbm, q_ref), (v_hbm, v_ref), (g_hbm, g_ref))
    loads = start_all([pltpu.make_async_copy(x, y, sem.at[i]) for i, (x, y) in enumerate(loads)])
    rb_pad[...] = jnp.zeros_like(rb_pad)
    rb_pad[0:HEADS, 0:BUCKETS] = rb_ref[...]
    for h in range(HEADS):
        for m, block in enumerate(bias_blocks(rb_pad[h : h + 1, :])):
            tab_ref[3 * h + m] = block
    wait_all(loads)
    for h in range(HEADS):
        hs = head(h)
        table = [tab_ref[3 * h + m] for m in range(3)]
        k = k_ref[:, hs]
        q = q_ref[2 * BLK :, hs]
        g = g_ref[2 * BLK :, hs]
        scores = [s * (SCALE * LOG2E) + t for s, t in zip(cut(dot(k, q, 1, 1)), table)]
        dp = cut(dot(v_ref[:, hs], g, 1, 1))
        expo, _, total, mixed = weights(scores, dp)
        inv = 1.0 / total
        prob, low, grad = softmax_grad(expo, dp, [inv] * 3, mixed * inv)
        low = stack(low)
        dq_ref[:, hs] = dot(low, k, 0, 0).astype(BF16)
        for i, out in enumerate((dot(low, q, 1, 0), dot(stack(prob), g, 1, 0))):
            mid_ref[i, :, hs] = out[: 2 * BLK]
            end_ref[i, :, hs] = out[2 * BLK :]
        pay_ref[2 * h : 2 * h + 2, :] = skew_sum(*grad)


def near_body(
    q_ref, k_ref, v_ref, g_ref, near_ref, tab_ref, pay_in,
    prob_ref, low_ref, pay_ref, expo_ref, dp_ref, stat_ref,
):
    hidden = hidden_keys()
    for h in range(HEADS):
        hs = head(h)
        table = [tab_ref[3 * h + m] for m in range(3)]
        q = q_ref[: 2 * BLK, hs]
        g = g_ref[: 2 * BLK, hs]
        raw = dot(stack([near_ref[0, :, hs], k_ref[: 2 * BLK, hs]]), q, 1, 1)
        dps = dot(stack([near_ref[1, :, hs], v_ref[: 2 * BLK, hs]]), g, 1, 1)
        scores = [s * (SCALE * LOG2E) + t for s, t in zip(cut(raw[LEAD:, BLK:]), [table[0] + hidden] + table[1:])]
        dp = cut(dps[LEAD:, BLK:])
        expo, _, total, mixed = weights(scores, dp)
        inv = 1.0 / total
        prob, low, grad = softmax_grad(expo, dp, [inv] * 3, mixed * inv)
        prob_ref[h] = stack(prob)
        low_ref[h] = stack(low)
        pay_ref[2 * h : 2 * h + 2, :] = skew_sum(*grad) + pay_in[2 * h : 2 * h + 2, :]
        shift = stack([table[0][FAR:] + hidden, table[1] + hidden, table[2]])
        rows = shift.shape[0]
        score = raw[:rows, :BLK] * (SCALE * LOG2E) + shift
        dp = dps[:rows, :BLK]
        peak = score.max(axis=0, keepdims=True)
        expo = jnp.exp2(score - peak)
        expo_ref[h] = expo
        dp_ref[h] = dp
        for i, x in enumerate((peak, sum_rows(expo), sum_rows(expo * dp))):
            stat_ref[3 * h + i : 3 * h + i + 1, :] = x


def far_body(
    q_ref, g_ref, far_ref, tab_ref, pay_in, expo_ref, dp_ref, stat_ref, prob1_ref, low1_ref,
    pay_hbm, prob_ref, low_ref, back_ref, pay_ref, sem,
):
    hidden = hidden_keys()
    pay = []
    for h in range(HEADS):
        hs = head(h)
        score = dot(far_ref[0, :, hs], q_ref[:BLK, hs], 1, 1) * (SCALE * LOG2E) + (tab_ref[3 * h, :FAR, :] + hidden)
        dp = dot(far_ref[1, :, hs], g_ref[:BLK, hs], 1, 1)
        peak, total, mixed = (stat_ref[3 * h + i : 3 * h + i + 1, :] for i in range(3))
        top = jnp.maximum(peak, score.max(axis=0, keepdims=True))
        expo = jnp.exp2(score - top)
        fade = jnp.exp2(peak - top)
        inv = 1.0 / (total * fade + sum_rows(expo))
        delta = (mixed * fade + sum_rows(expo * dp)) * inv
        prob = stack([expo * inv, expo_ref[h] * (fade * inv)])
        grad = prob * (stack([dp, dp_ref[h]]) - delta)
        prob_ref[h] = prob.astype(BF16)
        low_ref[h] = (grad * SCALE).astype(BF16)
        pay.append(skew_sum(*cut(grad)))
    total = jnp.concatenate(pay, axis=0) + pay_in[...]
    pay_ref[...] = jnp.broadcast_to(total[None], pay_ref.shape)
    copy = pltpu.make_async_copy(pay_ref, pay_hbm, sem)
    copy.start()

    def halo(h, carry):
        hs = pl.ds(pl.multiple_of(h * HEAD_DIM, HEAD_DIM), HEAD_DIM)
        pairs = ((low_ref, low1_ref, q_ref), (prob_ref, prob1_ref, g_ref))
        for i, (w0, w1, x) in enumerate(pairs):
            both = jnp.concatenate([w0[h, BLK : 2 * BLK, :], w1[h, :BLK, :]], axis=1)
            back_ref[i, :BLK, hs] = dot(w0[h, :BLK, :], x[:BLK, hs], 1, 0).astype(BF16)
            back_ref[i, BLK:, hs] = dot(both, x[: 2 * BLK, hs], 1, 0).astype(BF16)
        return carry

    lax.fori_loop(0, HEADS, halo, 0)
    copy.wait()


def join_body(
    q_ref, k_ref, g_ref, near_ref, far_ref, mid_ref, end_ref,
    prob_ref, low_ref, prob1_ref, low1_ref, dq2_ref, back_ref,
    dq_ref, dk_ref, dv_ref,
):
    dq_ref[2 * BLK :, :] = dq2_ref[...]
    for h in range(HEADS):
        hs = head(h)
        keys = stack([far_ref[0, :, hs], near_ref[0, :, hs], k_ref[: 2 * BLK, hs]])
        dq_ref[:BLK, hs] = dot(low_ref[h], keys[: 3 * BLK], 0, 0).astype(BF16)
        dq_ref[BLK : 2 * BLK, hs] = dot(low1_ref[h], keys[BLK:], 0, 0).astype(BF16)
        pairs = ((dk_ref, low_ref, low1_ref, q_ref), (dv_ref, prob_ref, prob1_ref, g_ref))
        for i, (out, w0, w1, x) in enumerate(pairs):
            both = jnp.concatenate([w0[h, 2 * BLK :, :], w1[h, BLK : 2 * BLK, :]], axis=1)
            first = dot(both, x[: 2 * BLK, hs], 1, 0) + mid_ref[i, :BLK, hs]
            second = dot(w1[h, 2 * BLK :, :], x[BLK : 2 * BLK, hs], 1, 0) + mid_ref[i, BLK:, hs]
            out[:BLK, hs] = first.astype(BF16)
            out[BLK : 2 * BLK, hs] = (second + back_ref[i, :BLK, hs].astype(F32)).astype(BF16)
            out[2 * BLK :, hs] = (end_ref[i, :, hs] + back_ref[i, BLK:, hs].astype(F32)).astype(BF16)


def table_body(x_order, c_order, x_ref, o_ref, sum_ref):
    heads = o_ref.shape[0]
    total = jnp.sum(x_ref[...], axis=0)
    cores = len(c_order)
    span = total.shape[0] // (len(x_order) * cores)
    for i, x in enumerate(x_order):
        for j, c in enumerate(c_order):
            at, to = (i * cores + j) * span, (x * cores + c) * span
            sum_ref[to : to + span, :] = total[at : at + span]
    low = sum_ref[pl.ds(0, heads, stride=2), :]
    mid = sum_ref[pl.ds(1, heads, stride=2), :]
    lane = lax.broadcasted_iota(jnp.int32, low.shape, 1)
    top = jnp.sum(jnp.where(lane < SEG, low, 0.0), axis=1, keepdims=True)
    mid = pltpu.roll(mid, SEG - 1, 1)
    first = jnp.where(lane < SEG - 1, pltpu.roll(low, SEG - 1, 1), mid)
    last = jnp.where(lane < SEG - 1, mid, top)
    o_ref[:, :BLK] = first
    o_ref[:, BLK:] = last[:, : BUCKETS - BLK]


def call(body, name, outs, args, spaces=None, scratch=(), mib=8, outputs=None):
    return pl.pallas_call(
        body,
        out_shape=tuple(jax.ShapeDtypeStruct(*o) for o in outs),
        in_specs=spaces or [VMEM] * len(args),
        out_specs=outputs or (VMEM,) * len(outs),
        scratch_shapes=scratch,
        compiler_params=pltpu.CompilerParams(vmem_limit_bytes=mib << 20),
        name=name,
    )(*args)


def late_first(count, order):
    return [i for i in order if i < count] + [i for i in range(count) if i not in order]


def exchange(x, size, outer, inner):
    rest = [a for a in AXES if a not in (outer[0], inner[0])]
    step = {a: math.prod(size[b] for b in AXES[AXES.index(a) + 1 :]) for a in AXES}
    groups = [
        [i * step[rest[0]] + j * step[rest[1]] + m * step[outer[0]] + n * step[inner[0]] for m in outer[1] for n in inner[1]]
        for i in range(size[rest[0]])
        for j in range(size[rest[1]])
    ]
    return lax.all_to_all(x, AXES, split_axis=0, concat_axis=0, axis_index_groups=groups, tiled=True)


def local(queries, keys, values, rel_bias, out_grad):
    _, rows, width = queries.shape
    q, k, v, g = (a.reshape(rows, width) for a in (queries, keys, values, out_grad))
    size = {a: lax.axis_size(a) for a in AXES}
    count = size["z"] * size["y"]
    pair = (2, BLK, width)
    q, k, v, g = (pltpu.with_memory_space_constraint(a, pltpu.HBM) for a in (q, k, v, g))
    near, far = call(
        tails_body,
        "tails",
        [((2, LEFT * SEG - FAR, width), BF16), ((2, FAR, width), BF16)],
        (k, v),
        [HBM] * 2,
        [pltpu.SemaphoreType.DMA((8,))],
        4,
    )
    ahead = [(s, s + 1) for s in range(count - 1)]
    near = lax.ppermute(near, ("z", "y"), ahead)
    far = lax.ppermute(far, ("z", "y"), ahead)
    q, k, v, g, dq2, mid, end, pay, table = call(
        own_body,
        "own",
        [((rows, width), BF16)] * 4
        + [
            ((BLK, width), BF16),
            ((2, 2 * BLK, width), F32),
            (pair, F32),
            ((2 * HEADS, BLK), F32),
            ((3 * HEADS, BLK, BLK), F32),
        ],
        (q, k, v, g, rel_bias),
        [HBM] * 4 + [VMEM],
        [pltpu.VMEM((8, 2 * BLK), F32), pltpu.SemaphoreType.DMA((4,))],
    )
    seen = (HEADS, 2 * BLK + LEAD, BLK)
    kept = ((HEADS, 3 * BLK, BLK), BF16)
    prob1, low1, pay, expo, dp, stat = call(
        near_body,
        "near",
        [kept, kept, ((2 * HEADS, BLK), F32), (seen, F32), (seen, F32), ((8, BLK), F32)],
        (q, k, v, g, near, table, pay),
    )
    group = size["y"] * size["c"]
    z_order, y_order, x_order, c_order = (late_first(size[a], ORDERS[a]) for a in AXES)
    pay, prob, low, back = call(
        far_body,
        "far",
        [
            ((group, 2 * HEADS, BLK), F32),
            kept,
            kept,
            ((2, 2 * BLK, width), BF16),
        ],
        (q, g, far, table, pay, expo, dp, stat, prob1, low1),
        scratch=[pltpu.VMEM((group, 2 * HEADS, BLK), F32), pltpu.SemaphoreType.DMA],
        outputs=(HBM, VMEM, VMEM, VMEM),
    )
    pay = exchange(pay, size, ("y", y_order), ("c", c_order))
    back = lax.ppermute(back, ("z", "y"), [(s + 1, s) for s in range(count - 1)])
    pay = pay.reshape(size["y"], size["c"] * 2 * HEADS, BLK).sum(axis=0)
    pay = jnp.broadcast_to(pay, (size["z"] * size["x"], *pay.shape))
    pay = exchange(pay, size, ("z", z_order), ("x", x_order))
    dq, dk, dv = call(
        join_body,
        "join",
        [((rows, width), BF16)] * 3,
        (q, k, g, near, far, mid, end, prob, low, prob1, low1, dq2, back),
    )
    (bias,) = call(
        functools.partial(table_body, x_order, c_order),
        "table",
        [((size["x"] * size["c"] * HEADS, BUCKETS), F32)],
        (pay.reshape(size["z"], size["x"] * size["c"] * 2 * HEADS, BLK),),
        scratch=[pltpu.VMEM((size["x"] * size["c"] * 2 * HEADS, BLK), F32)],
        mib=4,
    )
    return tuple(a.reshape(queries.shape) for a in (dq, dk, dv)) + (bias,)


def solution(mesh):
    sp, tp = mesh.devices.shape
    split = Mesh(mesh.devices.reshape(8, sp // 8, tp // 2, 2), AXES)
    rows = P(None, ("z", "y"), ("x", "c"))
    return jax.shard_map(
        local,
        mesh=split,
        in_specs=(rows, rows, rows, P(("x", "c"), None), rows),
        out_specs=(rows, rows, rows, P()),
        check_vma=False,
    )
```
